32 devices in a mesh: grp: 2 (over y), fs: 4 (over z), tp: 4 (over x, core).
Axes of the slice: x: 2, y: 2, z: 4, core: 2. Of those that a mesh axis runs over, the one named last changes fastest.
Arguments:
- tokens: bfloat16 [8192, 2048], P(('grp', 'fs', 'tp')), parts along dimension 0, may hold values from -6 to 6
- norm_gains: float32 [4, 2048], replicated, may hold values from 0.1 to 1.9
- query_weight: bfloat16 [2048, 2048], P('fs', 'tp'), may hold values from -0.125 to 0.125
- key_weight: bfloat16 [2048, 2048], P('fs', 'tp'), may hold values from -0.125 to 0.125
- value_weight: bfloat16 [2048, 4096], P('fs', 'tp'), may hold values from -0.125 to 0.125
- swish_weight: bfloat16 [2048, 4096], P('fs', 'tp'), may hold values from -0.125 to 0.125
- mixer_output: bfloat16 [4096, 2048], P('tp', 'fs'), may hold values from -0.09375 to 0.09375
- gate_weight: bfloat16 [2048, 3072], P('fs', 'tp'), may hold values from -0.125 to 0.125
- up_weight: bfloat16 [2048, 3072], P('fs', 'tp'), may hold values from -0.125 to 0.125
- down_weight: bfloat16 [3072, 2048], P('tp', 'fs'), may hold values from -0.109375 to 0.109375
Outputs:
- layer_output: bfloat16 [8192, 2048], P(('grp', 'fs', 'tp')), parts along dimension 0
The draws below stay inside these ranges and needn't reach their ends.
There are 2 independent parts, one for each index of `grp`. The reference program is written for one: setup_inputs(seed, part) draws one part's arguments, and reference() takes and returns one part's arrays. A program takes and returns all parts, laid end to end along the dimension named above; an argument that names none is the same for every part. Nothing has to cross between parts.
All inputs are finite; a program needn't handle non-finite values.
Results may differ from the reference program's by a relative error of at most 0.02.
Values may be sent and summed in bfloat16 or wider, within the bound.
A program may use at most 128 MiB of HBM per device.

```python
import jax
import jax.numpy as jnp
from jax import lax

D = 2048
H = 8
QK = 256
VD = 512
FF = 3072
BLOCK = 128
SEQ = 1024
TOKENS = 4096
N_TP = 4


def levels(own_key, shape, pieces, low, top_value):
    level, own = 1.0, jax.random.fold_in(own_key, 6)
    for dim, parts in pieces:
        draws = jnp.exp(jax.random.uniform(jax.random.fold_in(own, dim), (parts,), jnp.float32, low / len(pieces), top_value / len(pieces)))
        level = level * jnp.repeat(draws, shape[dim] // parts).reshape([-1 if axis == dim else 1 for axis in range(len(shape))])
    return level


def noise(key, extent, deviation, most, split=(), kind=jnp.bfloat16):
    level = levels(key, extent, split, -0.22, 0.18) if split else 1.0
    array = jax.random.normal(key, extent, jnp.float32) * deviation * level
    return jnp.minimum(jnp.maximum(array, -most), most).astype(kind)


def setup_inputs(seed: int = 0, part: int = 0) -> dict:
    key_of = jax.random.split(jax.random.key(seed), 11)
    part_splits = jax.random.split(jax.random.fold_in(key_of[10], part), 11)
    tokens = noise(part_splits[0], (TOKENS, D), 1.0, 6.0, ((0, 16),))
    norm_gains = jnp.clip(1.0 + 0.18 * jax.random.normal(key_of[1], (4, D), jnp.float32), 0.1, 1.9)
    query_weight = noise(key_of[2], (D, H * QK), D ** -0.5, 0.125, ((0, 4), (1, 4)))
    key_weight = noise(key_of[3], (D, H * QK), D ** -0.5, 0.125, ((0, 4), (1, 4)))
    value_weight = noise(key_of[4], (D, H * VD), D ** -0.5, 0.125, ((0, 4), (1, 4)))
    swish_weight = noise(key_of[5], (D, H * VD), D ** -0.5, 0.125, ((0, 4), (1, 4)))
    mixer_output = noise(key_of[6], (H * VD, D), (H * VD) ** -0.5, 0.09375, ((0, 4), (1, 4)))
    gate_weight = noise(key_of[7], (D, FF), D ** -0.5, 0.125, ((0, 4), (1, 4)))
    up_weight = noise(key_of[8], (D, FF), D ** -0.5, 0.125, ((0, 4), (1, 4)))
    down_weight = noise(key_of[9], (FF, D), FF ** -0.5, 0.109375, ((0, 4), (1, 4)))
    return dict(tokens=tokens, norm_gains=norm_gains, query_weight=query_weight, key_weight=key_weight, value_weight=value_weight, swish_weight=swish_weight, mixer_output=mixer_output, gate_weight=gate_weight, up_weight=up_weight, down_weight=down_weight)


norm_epsilon = 1e-06
group_epsilon = 0.01

def rms_scale(matrix, gain):
    return matrix * lax.rsqrt(lax.optimization_barrier(jnp.mean(matrix * matrix, axis=-1, keepdims=True)) + norm_epsilon) * gain

def rotate_halves(head_tensors, cosine_table, sine_table):
    half_width = head_tensors.shape[-1] // 2
    lower_half = head_tensors[..., :half_width]
    upper_half = head_tensors[..., half_width:]
    return jnp.concatenate([lower_half * cosine_table - upper_half * sine_table, lower_half * sine_table + upper_half * cosine_table], axis=-1)

def decayed_sum(queries, key_rows, value_rows, log_decay):
    query_expanded = queries.astype(jnp.float32)
    key_expanded = key_rows.astype(jnp.float32)
    value_wide = value_rows.astype(jnp.float32)
    retention_scores = jnp.einsum('fzy,czy->zfc', query_expanded, key_expanded)
    offsets = jnp.arange(queries.shape[0], dtype=jnp.float32)
    distance = offsets[:, None] - offsets[None, :]
    weights = jnp.where(distance >= 0, jnp.exp(log_decay[:, None, None] * jnp.maximum(distance, 0.0)), 0.0)
    return jnp.einsum('hnm,mhe->nhe', retention_scores * weights, value_wide)

def grouped_product(active, weight):
    group_width = active.shape[1] // N_TP
    running = jnp.zeros((active.shape[0], weight.shape[1]), jnp.float32)
    for group_index in range(N_TP):
        lower = group_index * group_width
        product = jnp.dot(active[:, lower:lower + group_width], weight[lower:lower + group_width], preferred_element_type=jnp.float32)
        rounded = lax.optimization_barrier(product.astype(jnp.bfloat16))
        running = running + rounded.astype(jnp.float32)
    return running

def reference(tokens, norm_gains, query_weight, key_weight, value_weight, swish_weight, mixer_output, gate_weight, up_weight, down_weight):
    residual = tokens.astype(jnp.float32)
    normed = rms_scale(residual, norm_gains[0]).astype(jnp.bfloat16)
    raw_query = jnp.dot(normed, query_weight, preferred_element_type=jnp.float32)
    raw_keys = jnp.dot(normed, key_weight, preferred_element_type=jnp.float32)
    raw_values = jnp.dot(normed, value_weight, preferred_element_type=jnp.float32)
    raw_swish = jnp.dot(normed, swish_weight, preferred_element_type=jnp.float32)
    seq_count = tokens.shape[0] // SEQ
    positions = jnp.arange(SEQ, dtype=jnp.float32)
    frequency = 10000.0 ** (-jnp.linspace(0.0, 1.0, QK // 2, dtype=jnp.float32))
    angles = positions[:, None] * frequency[None, :]
    cosine_table = jnp.cos(angles)[:, None, :]
    sine_table = jnp.sin(angles)[:, None, :]
    queries = rotate_halves(raw_query.reshape(seq_count, SEQ, H, QK), cosine_table, sine_table).astype(jnp.bfloat16)
    key_rows = (rotate_halves(raw_keys.reshape(seq_count, SEQ, H, QK), cosine_table, sine_table) * QK ** (-0.5)).astype(jnp.bfloat16)
    value_rows = raw_values.reshape(seq_count, SEQ, H, VD).astype(jnp.bfloat16)
    head_index = jnp.arange(H, dtype=jnp.float32)
    log_decay = -(4.0 / BLOCK) * (BLOCK / (32.0 * SEQ)) ** (head_index / (H - 1))
    retained = lax.map(lambda triple: decayed_sum(triple[0], triple[1], triple[2], log_decay), (queries, key_rows, value_rows))
    centred = retained - lax.optimization_barrier(jnp.mean(retained, axis=-1, keepdims=True))
    normalized = centred * lax.rsqrt(lax.optimization_barrier(jnp.mean(centred * centred, axis=-1, keepdims=True)) + group_epsilon)
    gated_rows = (jax.nn.silu(raw_swish) * normalized.reshape(tokens.shape[0], H * VD)).astype(jnp.bfloat16)
    mixer_total = grouped_product(gated_rows, mixer_output)
    after_mixer = residual + rms_scale(mixer_total, norm_gains[1])
    widened = rms_scale(after_mixer, norm_gains[2]).astype(jnp.bfloat16)
    gate_sum = jnp.dot(widened, gate_weight, preferred_element_type=jnp.float32)
    up_sum = jnp.dot(widened, up_weight, preferred_element_type=jnp.float32)
    hidden = (jax.nn.silu(gate_sum) * up_sum).astype(jnp.bfloat16)
    channel = grouped_product(hidden, down_weight)
    return (after_mixer + rms_scale(channel, norm_gains[3])).astype(jnp.bfloat16)
```

```python
import functools
import math

import jax
import jax.numpy as jnp
from jax import lax
from jax.experimental import pallas as pl
from jax.experimental.pallas import tpu as pltpu
from jax.sharding import PartitionSpec as P

QK = 256
BLOCK = 128
CORES = 2

norm_epsilon = 1e-06
group_epsilon = 0.01

MESH = pl.DeviceIdType.MESH
f32, bf16 = jnp.float32, jnp.bfloat16

WQ, WK, WV, WS, WM, WG, WU, WD = range(8)


def rms(matrix):
    return matrix * lax.rsqrt(jnp.mean(matrix * matrix, axis=-1, keepdims=True) + norm_epsilon)


def silu(value):
    return value / (1.0 + jnp.exp(-value))


def dot(left, right):
    return jnp.dot(left, right, preferred_element_type=f32)


def ds(start, size, multiple=None):
    return pl.ds(pl.multiple_of(start, multiple or size), size)


def layer(G, F, T, *refs):
    tokens, gains, cosine, sine = refs[:4]
    shards = refs[4:12]
    out = refs[12]
    bufs = refs[13:21]
    (act, queries, keys, values, swish, gated, after, total, send1, recv1, send2, recv2) = refs[21:33]
    (local_sem, z_send, z_recv, y_send, y_recv, ag_x_send, ag_x_recv, ag_c_send, ag_c_recv,
     rs1_send, rs1_recv, rs2_send, rs2_recv) = refs[33:]

    X = T // CORES
    g, f, t = lax.axis_index("grp"), lax.axis_index("fs"), lax.axis_index("tp")
    x, c = t // CORES, t % CORES
    R, D = tokens.shape
    L = R * T
    TM = min(256, L)
    heads = queries.shape[1] // QK
    VD = values.shape[1] // heads
    FH = bufs[WG].shape[1]
    partner = (g, f, x * CORES + (1 - c))

    def x_peer(o):
        return lax.rem(x + o, X)

    neighbours = [(f > 0, (g, f - 1, t)), (f < F - 1, (g, f + 1, t))]
    neighbours += [(None, (lax.rem(g + o, G), f, t)) for o in range(1, G)]
    neighbours += [(None, (g, f, x_peer(o) * CORES + c)) for o in range(1, X)]
    neighbours += [(None, partner)]

    def when(condition, action):
        if condition is None:
            action()
        else:
            pl.when(condition)(action)

    def local_copy(w):
        r = shards[w].shape[0]
        return pltpu.make_async_copy(shards[w], bufs[w].at[ds(f * r, r)], local_sem.at[w])

    def half(w, s, part):
        r = shards[w].shape[0]
        return bufs[w].at[ds(s * r + part * (r // G), r // G)]

    def source(d, k):
        return (f - k if d == 0 else f + k)

    def valid(d, k):
        return (f >= k if d == 0 else f + k < F)

    def z_copy(w, k, d):
        region = half(w, source(d, k), g)
        return pltpu.make_async_remote_copy(
            region, region, z_send.at[d, w, k], z_recv.at[d, w, k + 1],
            device_id=(g, f + 1 if d == 0 else f - 1, t), device_id_type=MESH)

    def z_wait(w, k, d):
        region = half(w, source(d, k), g)
        pltpu.make_async_remote_copy(
            region, region, z_send.at[d, w, k], z_recv.at[d, w, k],
            device_id=(g, f, t), device_id_type=MESH).wait_recv()

    def y_copy(w, k, d, o):
        region = half(w, source(d, k), g)
        return pltpu.make_async_remote_copy(
            region, region, y_send.at[d, w, k, o], y_recv.at[d, w, k, o],
            device_id=(lax.rem(g + o, G), f, t), device_id_type=MESH)

    def y_wait(w, k, d, o):
        region = half(w, source(d, k), lax.rem(g + G - o, G))
        pltpu.make_async_remote_copy(
            region, region, y_send.at[d, w, k, o], y_recv.at[d, w, k, o],
            device_id=(g, f, t), device_id_type=MESH).wait_recv()

    def has_next(d):
        return f < F - 1 if d == 0 else f > 0

    def comm(w, k):
        if k == 0:
            local_copy(w).wait()
        for d in range(2):
            if k == 0:
                pl.when(has_next(d))(lambda d=d: z_copy(w, k, d).start())
            else:
                @pl.when(valid(d, k))
                def _(d=d):
                    z_wait(w, k, d)
                    if k < F - 1:
                        pl.when(has_next(d))(lambda: z_copy(w, k, d).start())
                    for o in range(1, G):
                        y_copy(w, k, d, o).start()

    def arrived(w):
        for k in range(1, F):
            for d in range(2):
                @pl.when(valid(d, k))
                def _(k=k, d=d):
                    for o in range(1, G):
                        y_wait(w, k, d, o)

    def drain(w):
        for k in range(F):
            for d in range(2):
                @pl.when(valid(d, k))
                def _(k=k, d=d):
                    if k < F - 1:
                        pl.when(has_next(d))(lambda: z_copy(w, k, d).wait_send())
                    if k > 0:
                        for o in range(1, G):
                            y_copy(w, k, d, o).wait_send()

    def rows_of(device):
        return act.at[ds(device * R, R)]

    def ag_x(stage, o):
        region = rows_of(t)
        return pltpu.make_async_remote_copy(
            region, region, ag_x_send.at[stage, o], ag_x_recv.at[stage, o],
            device_id=(g, f, x_peer(o) * CORES + c), device_id_type=MESH)

    def ag_c(stage, o, core):
        region = rows_of(x_peer(X - o) * CORES + core)
        return pltpu.make_async_remote_copy(
            region, region, ag_c_send.at[stage, o], ag_c_recv.at[stage, o],
            device_id=partner, device_id_type=MESH)

    def gather_start(stage):
        for o in range(1, X):
            ag_x(stage, o).start()
        ag_c(stage, 0, c).start()

    def gather_forward(stage):
        for o in range(1, X):
            region = rows_of(x_peer(X - o) * CORES + c)
            pltpu.make_async_remote_copy(
                region, region, ag_x_send.at[stage, o], ag_x_recv.at[stage, o],
                device_id=(g, f, t), device_id_type=MESH).wait_recv()
            ag_c(stage, o, c).start()

    def gather_wait(stage):
        for o in range(X):
            ag_c(stage, o, 1 - c).wait_recv()

    def gather_drain(stage):
        for o in range(X):
            if o:
                ag_x(stage, o).wait_send()
            ag_c(stage, o, c).wait_send()

    def rs1(stage, j):
        return pltpu.make_async_remote_copy(
            send1.at[j], recv1.at[j], rs1_send.at[stage, j], rs1_recv.at[stage, j],
            device_id=partner, device_id_type=MESH)

    def rs2(stage, j, o):
        return pltpu.make_async_remote_copy(
            send2.at[j, o], recv2.at[j, o], rs2_send.at[stage, j, o], rs2_recv.at[stage, j, o],
            device_id=(g, f, x_peer(o) * CORES + c), device_id_type=MESH)

    def partial_rows(w, width, j, device):
        r = shards[w].shape[0]
        return dot(gated[ds(device * R, R), :width], bufs[w][ds(j * r, r), :])

    def sum_send(stage, w, width, j):
        def one(o, _):
            send1[j, o] = partial_rows(w, width, j, o * CORES + (1 - c)).astype(bf16)
            return 0
        lax.fori_loop(0, X, one, 0)
        rs1(stage, j).start()

    def sum_pass(stage, w, width, j):
        cols = send1.shape[-1]
        rs1(stage, j).wait_recv()
        def pair(o):
            peer = x_peer(o)
            return partial_rows(w, width, j, peer * CORES + c) + recv1[j, peer].astype(f32)
        for o in range(1, X):
            send2[j, o] = pair(o).astype(bf16)
            rs2(stage, j, o).start()
        total[:, ds(j * cols, cols)] = pair(0)

    def sum_finish(stage):
        cols = send1.shape[-1]
        def one(j, _):
            for o in range(1, X):
                rs2(stage, j, o).wait_recv()
                total[:, ds(j * cols, cols)] += recv2[j, o].astype(f32)
            return 0
        lax.fori_loop(0, F, one, 0)

    def sum_drain(stage):
        def one(j, _):
            rs1(stage, j).wait_send()
            for o in range(1, X):
                rs2(stage, j, o).wait_send()
            return 0
        lax.fori_loop(0, F, one, 0)

    RT = min(32, R)

    def norm_in():
        def one(i, _):
            rows = ds(i * RT, RT)
            act[ds(t * R + i * RT, RT)] = (
                rms(tokens[rows].astype(f32)) * gains[0:1]).astype(bf16)
            return 0
        lax.fori_loop(0, R // RT, one, 0)

    def norm_mid():
        def one(i, _):
            rows = ds(i * RT, RT)
            mid = tokens[rows].astype(f32) + rms(total[rows]) * gains[1:2]
            after[rows] = mid
            act[ds(t * R + i * RT, RT)] = (rms(mid) * gains[2:3]).astype(bf16)
            return 0
        lax.fori_loop(0, R // RT, one, 0)

    def norm_out():
        def one(i, _):
            rows = ds(i * RT, RT)
            out[rows] = (after[rows] + rms(total[rows]) * gains[3:4]).astype(bf16)
            return 0
        lax.fori_loop(0, R // RT, one, 0)

    def tiles(width, tile, body):
        across = width // tile

        def one(i, _):
            body(ds((i // across) * TM, TM), ds((i % across) * tile, tile))
            return 0
        lax.fori_loop(0, (L // TM) * across, one, 0)

    def rotary(w, into, scale):
        def body(rows, cols):
            head = dot(act[rows], bufs[w][:, cols])
            lower, upper = head[:, :QK // 2], head[:, QK // 2:]
            cos, sin = cosine[rows], sine[rows]
            rotated = jnp.concatenate(
                [lower * cos - upper * sin, lower * sin + upper * cos], axis=-1)
            into[rows, cols] = (rotated * scale).astype(bf16)
        tiles(heads * QK, QK, body)

    def project(w, into):
        def body(rows, cols):
            into[rows, cols] = dot(act[rows], bufs[w][:, cols]).astype(into.dtype)
        tiles(heads * VD, VD, body)

    def retain(h):
        head_index = (t * heads + h).astype(f32)
        fraction = jnp.full((1, 1), 1.0, f32) * (head_index / (heads * T - 1.0))
        log_decay = -(4.0 / BLOCK) * jnp.exp(fraction * math.log(BLOCK / (32.0 * L)))
        qk_cols = ds(h * QK, QK)
        v_cols = ds(h * VD, VD)
        for i in range(L // TM):
            rows, seen = pl.ds(i * TM, TM), (i + 1) * TM
            scores = lax.dot_general(
                queries[rows, qk_cols], keys[:seen, qk_cols], (((1,), (1,)), ((), ())),
                preferred_element_type=f32)
            distance = (lax.broadcasted_iota(jnp.int32, (TM, seen), 0) + i * TM
                        - lax.broadcasted_iota(jnp.int32, (TM, seen), 1)).astype(f32)
            weights = jnp.where(
                distance >= 0, jnp.exp(log_decay * jnp.maximum(distance, 0.0)), 0.0)
            retained = dot((scores * weights).astype(bf16), values[:seen, v_cols])
            centred = retained - jnp.mean(retained, axis=-1, keepdims=True)
            normalized = centred * lax.rsqrt(
                jnp.mean(centred * centred, axis=-1, keepdims=True) + group_epsilon)
            gated[rows, v_cols] = (silu(swish[rows, v_cols]) * normalized).astype(bf16)

    def hidden_units():
        def body(rows, cols):
            up = dot(act[rows], bufs[WU][:, cols])
            gate = dot(act[rows], bufs[WG][:, cols])
            gated[rows, cols] = (silu(gate) * up).astype(bf16)
        tiles(FH, math.gcd(FH, 256), body)

    for w in range(8):
        local_copy(w).start()
    barrier = pltpu.get_barrier_semaphore()
    for condition, device in neighbours:
        when(condition, lambda device=device: pl.semaphore_signal(
            barrier, inc=1, device_id=device, device_id_type=MESH))
    fixed = (G - 1) + (X - 1) + 1
    pl.semaphore_wait(
        barrier, fixed + (f > 0).astype(jnp.int32) + (f < F - 1).astype(jnp.int32))

    comm(WQ, 0)
    comm(WK, 0)
    norm_in()
    gather_start(0)
    for k in range(1, F):
        comm(WQ, k)
    comm(WV, 0)
    comm(WK, 1)
    gather_forward(0)
    for k in range(2, F):
        comm(WK, k)
    comm(WS, 0)
    gather_wait(0)
    arrived(WQ)
    rotary(WQ, queries, 1.0)
    comm(WV, 1)
    arrived(WK)
    rotary(WK, keys, QK ** -0.5)
    for k in range(2, F):
        comm(WV, k)
    comm(WM, 0)
    comm(WS, 1)
    arrived(WV)
    project(WV, values)
    for k in range(2, F):
        comm(WS, k)
    comm(WG, 0)
    comm(WM, 1)
    arrived(WS)
    project(WS, swish)
    gather_drain(0)
    if F > 2:
        comm(WM, 2)
    lax.fori_loop(0, heads, lambda h, _: (retain(h), 0)[1], 0)
    for k in range(3, F):
        comm(WM, k)
    comm(WU, 0)
    arrived(WM)

    def mixer(j, _):
        pl.when(j < F)(lambda: sum_send(0, WM, heads * VD, jnp.minimum(j, F - 1)))
        pl.when(j > 0)(lambda: sum_pass(0, WM, heads * VD, jnp.maximum(j - 1, 0)))
        return 0
    lax.fori_loop(0, F + 1, mixer, 0)
    for k in range(1, F):
        comm(WG, k)
    comm(WD, 0)
    sum_finish(0)
    norm_mid()
    gather_start(1)
    for k in range(1, F):
        comm(WU, k)
    gather_forward(1)
    comm(WD, 1)
    gather_wait(1)
    arrived(WG)
    arrived(WU)
    sum_drain(0)
    hidden_units()

    def down(j, first, second):
        if first:
            sum_send(1, WD, FH, j)
        if second:
            sum_pass(1, WD, FH, j)
    down(f, True, True)
    for k in range(1, F):
        if k > 1:
            comm(WD, k)
        for d in range(2):
            @pl.when(valid(d, k))
            def _(k=k, d=d):
                for o in range(1, G):
                    y_wait(WD, k, d, o)
                sum_send(1, WD, FH, source(d, k))
                sum_pass(1, WD, FH, source(d, k))
    sum_finish(1)
    norm_out()
    gather_drain(1)
    sum_drain(1)
    for w in range(8):
        drain(w)


def per_device(tokens, norm_gains, *weights):
    G, F, T = lax.axis_size("grp"), lax.axis_size("fs"), lax.axis_size("tp")
    X = T // CORES
    R, D = tokens.shape
    L = R * T
    query, _, value, _, mixer, gate, _, down = weights
    qk_width, v_width, hidden = query.shape[1], value.shape[1], gate.shape[1]
    positions = jnp.arange(L, dtype=f32)
    frequency = 10000.0 ** (-jnp.linspace(0.0, 1.0, QK // 2, dtype=f32))
    angles = positions[:, None] * frequency[None, :]
    vmem = pl.BlockSpec(memory_space=pltpu.VMEM)
    anywhere = pl.BlockSpec(memory_space=pl.ANY)
    DMA = pltpu.SemaphoreType.DMA
    cols = mixer.shape[1]
    scratch = [pltpu.VMEM((w.shape[0] * F, w.shape[1]), bf16) for w in weights]
    scratch += [
        pltpu.VMEM((L, D), bf16),
        pltpu.VMEM((L, qk_width), bf16),
        pltpu.VMEM((L, qk_width), bf16),
        pltpu.VMEM((L, v_width), bf16),
        pltpu.VMEM((L, v_width), f32),
        pltpu.VMEM((L, max(v_width, hidden)), bf16),
        pltpu.VMEM((R, D), f32),
        pltpu.VMEM((R, D), f32),
        pltpu.VMEM((F, X, R, cols), bf16),
        pltpu.VMEM((F, X, R, cols), bf16),
        pltpu.VMEM((F, X, R, cols), bf16),
        pltpu.VMEM((F, X, R, cols), bf16),
        DMA((8,)),
        DMA((2, 8, F)), DMA((2, 8, F)), DMA((2, 8, F, G)), DMA((2, 8, F, G)),
        DMA((2, X)), DMA((2, X)), DMA((2, X)), DMA((2, X)),
        DMA((2, F)), DMA((2, F)), DMA((2, F, X)), DMA((2, F, X)),
    ]
    return pl.pallas_call(
        functools.partial(layer, G, F, T),
        out_shape=jax.ShapeDtypeStruct((R, D), bf16),
        in_specs=[vmem] * 4 + [anywhere] * 8,
        out_specs=vmem,
        scratch_shapes=scratch,
        compiler_params=pltpu.CompilerParams(
            collective_id=0, has_side_effects=True, vmem_limit_bytes=67043328),
    )(tokens, norm_gains, jnp.cos(angles), jnp.sin(angles), *weights)


def solution(mesh):
    placed = (
        P(("grp", "fs", "tp"), None),
        P(),
        P("fs", "tp"),
        P("fs", "tp"),
        P("fs", "tp"),
        P("fs", "tp"),
        P("tp", "fs"),
        P("fs", "tp"),
        P("fs", "tp"),
        P("tp", "fs"),
    )
    return jax.shard_map(
        per_device,
        mesh=mesh,
        in_specs=placed,
        out_specs=P(("grp", "fs", "tp"), None),
        check_vma=False,
    )
```

```python
import functools
import math

import jax
import jax.numpy as jnp
from jax import lax
from jax.experimental import pallas as pl
from jax.experimental.pallas import tpu as pltpu
from jax.sharding import PartitionSpec as P

QK = 256
BLOCK = 128
CORES = 2

norm_epsilon = 1e-06
group_epsilon = 0.01

MESH = pl.DeviceIdType.MESH
f32, bf16 = jnp.float32, jnp.bfloat16

WQ, WK, WV, WS, WM, WG, WU, WD = range(8)


def rms(matrix):
    return matrix * lax.rsqrt(jnp.mean(matrix * matrix, axis=-1, keepdims=True) + norm_epsilon)


def silu(value):
    return value / (1.0 + jnp.exp(-value))


def dot(left, right):
    return jnp.dot(left, right, preferred_element_type=f32)


def ds(start, size, multiple=None):
    return pl.ds(pl.multiple_of(start, multiple or size), size)


MIXER = (WQ, WK, WV, WS, WM)
WHOLE = (WQ, WK, WV, WS, WG, WU, WD)


def layer(G, F, T, *refs):
    tokens, gains, cosine, sine = refs[:4]
    shards = refs[4:12]
    out = refs[12]
    bufs = refs[13:21]
    act, queries, keys, values, acc, send1, recv1, recv2 = refs[21:29]
    (local_sem, z_send, z_recv, y_send, y_recv, e_send, e_recv, ag_x_send, ag_x_recv, ag_c_send,
     ag_c_recv, rs1_send, rs1_recv, rs2_send, rs2_recv, client_sem, ret_send, ret_recv) = refs[29:]

    X = T // CORES
    g, f, t = lax.axis_index("grp"), lax.axis_index("fs"), lax.axis_index("tp")
    x, c = t // CORES, t % CORES
    R, D = tokens.shape
    L = R * T
    TM = min(256, L)
    heads = queries.shape[2] // QK
    VD = values.shape[2] // heads
    FH = bufs[WG].shape[1]
    total, after = acc.at[0], acc.at[1]
    partner = (g, f, x * CORES + (1 - c))

    moved = F >= 4
    is_end = (f == 0) | (f == F - 1) if moved else f < 0
    is_host = (f == 1) | (f == F - 2) if moved else f < 0
    not_end = jnp.logical_not(is_end)
    outer = jnp.where(f == 1, 0, F - 1)
    host = jnp.where(f == 0, 1, F - 2)

    def x_peer(o):
        return lax.rem(x + o, X)

    neighbours = [(f > 0, (g, f - 1, t)), (f < F - 1, (g, f + 1, t))]
    neighbours += [(None, (lax.rem(g + o, G), f, t)) for o in range(1, G)]
    neighbours += [(None, (g, f, x_peer(o) * CORES + c)) for o in range(1, X)]
    neighbours += [(None, partner)]

    def when(condition, action):
        if condition is None:
            action()
        else:
            pl.when(condition)(action)

    def local_copy(w):
        r = shards[w].shape[0]
        return pltpu.make_async_copy(shards[w], bufs[w].at[ds(f * r, r)], local_sem.at[w])

    def half(w, s, part):
        r = shards[w].shape[0]
        return bufs[w].at[ds(s * r + part * (r // G), r // G)]

    def source(d, k):
        return (f - k if d == 0 else f + k)

    def valid(d, k):
        return (f >= k if d == 0 else f + k < F)

    def has_next(w, d):
        margin = 1 if moved and w in MIXER else 0
        return f < F - 1 - margin if d == 0 else f > margin

    def takes(w, k, d):
        return valid(d, k) & not_end if w in MIXER else valid(d, k)

    def gives(w, k, d):
        return has_next(w, d) if k == 0 else takes(w, k, d) & has_next(w, d)

    def outward(d):
        return is_host & (f == F - 2 if d == 0 else f == 1)

    def from_end(d):
        return is_host & (f == 1 if d == 0 else f == F - 2)

    def crosses(w, k, d):
        if w in WHOLE and k == 1:
            return takes(w, k, d) & jnp.logical_not(from_end(d))
        return takes(w, k, d)

    def z_copy(w, k, d):
        region = half(w, source(d, k), g)
        return pltpu.make_async_remote_copy(
            region, region, z_send.at[d, w, k], z_recv.at[d, w, k + 1],
            device_id=(g, f + 1 if d == 0 else f - 1, t), device_id_type=MESH)

    def z_wait(w, k, d):
        region = half(w, source(d, k), g)
        pltpu.make_async_remote_copy(
            region, region, z_send.at[d, w, k], z_recv.at[d, w, k],
            device_id=(g, f, t), device_id_type=MESH).wait_recv()

    def y_copy(w, k, d, o):
        region = half(w, source(d, k), g)
        return pltpu.make_async_remote_copy(
            region, region, y_send.at[d, w, k, o], y_recv.at[d, w, k, o],
            device_id=(lax.rem(g + o, G), f, t), device_id_type=MESH)

    def y_wait(w, k, d, o):
        region = half(w, source(d, k), lax.rem(g + G - o, G))
        pltpu.make_async_remote_copy(
            region, region, y_send.at[d, w, k, o], y_recv.at[d, w, k, o],
            device_id=(g, f, t), device_id_type=MESH).wait_recv()

    def end_copy(w, o, s, device):
        region = half(w, s, lax.rem(g + o, G))
        return pltpu.make_async_remote_copy(
            region, region, e_send.at[w, o], e_recv.at[w, o],
            device_id=(g, device, t), device_id_type=MESH)

    def give_own(w, early):
        for d in range(2):
            if w in MIXER:
                condition = has_next(w, d)
            elif early:
                condition = outward(d)
            else:
                condition = has_next(w, d) & jnp.logical_not(outward(d))
            pl.when(condition)(lambda d=d: z_copy(w, 0, d).start())
        if w in WHOLE and not early:
            @pl.when(is_end)
            def _():
                for o in range(1, G):
                    end_copy(w, o, f, host).start()

    def comm(w, k):
        if k == 0:
            if w in MIXER:
                local_copy(w).wait()
            give_own(w, False)
            return
        for d in range(2):
            @pl.when(takes(w, k, d))
            def _(d=d):
                z_wait(w, k, d)
                if k < F - 1:
                    pl.when(has_next(w, d))(lambda: z_copy(w, k, d).start())
            @pl.when(crosses(w, k, d))
            def _(d=d):
                for o in range(1, G):
                    y_copy(w, k, d, o).start()

    def arrived_from(w, k, d):
        @pl.when(crosses(w, k, d))
        def _():
            for o in range(1, G):
                y_wait(w, k, d, o)
        if w in WHOLE and k == 1:
            @pl.when(from_end(d))
            def _():
                for o in range(1, G):
                    end_copy(w, o, source(d, k), f).wait_recv()

    def arrived(w):
        for k in range(1, F):
            for d in range(2):
                arrived_from(w, k, d)

    def drain(w):
        for k in range(F):
            for d in range(2):
                if k < F - 1:
                    pl.when(gives(w, k, d))(lambda k=k, d=d: z_copy(w, k, d).wait_send())
                if k > 0:
                    @pl.when(crosses(w, k, d))
                    def _(k=k, d=d):
                        for o in range(1, G):
                            y_copy(w, k, d, o).wait_send()
        if w in WHOLE:
            @pl.when(is_end)
            def _():
                for o in range(1, G):
                    end_copy(w, o, f, host).wait_send()

    def rows_of(q, device):
        return act.at[q, ds(device * R, R)]

    def slot(stage):
        return 1 if stage == 1 else 0

    def ag_x(stage, o):
        region = rows_of(slot(stage), t)
        return pltpu.make_async_remote_copy(
            region, region, ag_x_send.at[stage, o], ag_x_recv.at[stage, o],
            device_id=(g, f, x_peer(o) * CORES + c), device_id_type=MESH)

    def ag_c(stage, o, core):
        region = rows_of(slot(stage), x_peer(X - o) * CORES + core)
        return pltpu.make_async_remote_copy(
            region, region, ag_c_send.at[stage, o], ag_c_recv.at[stage, o],
            device_id=partner, device_id_type=MESH)

    def gather_start(stage):
        for o in range(1, X):
            ag_x(stage, o).start()
        ag_c(stage, 0, c).start()

    def gather_forward(stage):
        for o in range(1, X):
            region = rows_of(slot(stage), x_peer(X - o) * CORES + c)
            pltpu.make_async_remote_copy(
                region, region, ag_x_send.at[stage, o], ag_x_recv.at[stage, o],
                device_id=(g, f, t), device_id_type=MESH).wait_recv()
            ag_c(stage, o, c).start()

    def gather_wait(stage):
        for o in range(X):
            ag_c(stage, o, 1 - c).wait_recv()

    def gather_drain(stage):
        for o in range(X):
            if o:
                ag_x(stage, o).wait_send()
            ag_c(stage, o, c).wait_send()

    def client_copy(device):
        return pltpu.make_async_remote_copy(
            rows_of(0, t), rows_of(1, t), client_sem.at[0], client_sem.at[1],
            device_id=(g, device, t), device_id_type=MESH)

    cols = send1.shape[-1]

    def rs1(stage, q, j):
        return pltpu.make_async_remote_copy(
            send1.at[q, j], recv1.at[q, j], rs1_send.at[stage, j], rs1_recv.at[stage, j],
            device_id=partner, device_id_type=MESH)

    def rs2(stage, q, j, o):
        return pltpu.make_async_remote_copy(
            send1.at[q, j, o], recv2.at[q, j, o], rs2_send.at[stage, j, o],
            rs2_recv.at[stage, j, o],
            device_id=(g, f, x_peer(o) * CORES + c), device_id_type=MESH)

    def give_back(j, device):
        return pltpu.make_async_remote_copy(
            send1.at[1, j, 0], recv2.at[0, j, 0], ret_send.at[j], ret_recv.at[j],
            device_id=(g, device, t), device_id_type=MESH)

    def partial_rows(w, width, q, j, device):
        r = shards[w].shape[0]
        return dot(values[q, ds(device * R, R), :width], bufs[w][ds(j * r, r), :])

    def sum_send(stage, q, w, width, j):
        def one(o, _):
            send1[q, j, o] = partial_rows(w, width, q, j, o * CORES + (1 - c)).astype(bf16)
            return 0
        lax.fori_loop(0, X, one, 0)
        rs1(stage, q, j).start()

    def sum_pass(stage, q, w, width, j):
        rs1(stage, q, j).wait()
        def pair(o):
            peer = x_peer(o)
            return (partial_rows(w, width, q, j, peer * CORES + c)
                    + recv1[q, j, peer].astype(f32))
        for o in range(1, X):
            send1[q, j, o] = pair(o).astype(bf16)
            rs2(stage, q, j, o).start()
        acc[q, :, ds(j * cols, cols)] = pair(0)

    def sum_finish(stage, q, j):
        block = acc[q, :, ds(j * cols, cols)]
        for o in range(1, X):
            rs2(stage, q, j, o).wait_recv()
            block += recv2[q, j, o].astype(f32)
        return block

    def sum_drain(stage, q):
        def one(j, _):
            for o in range(1, X):
                rs2(stage, q, j, o).wait_send()
            return 0
        lax.fori_loop(0, F, one, 0)

    RT = min(32, R)

    def norm_in():
        def one(i, _):
            rows = ds(i * RT, RT)
            act[0, ds(t * R + i * RT, RT)] = (
                rms(tokens[rows].astype(f32)) * gains[0:1]).astype(bf16)
            return 0
        lax.fori_loop(0, R // RT, one, 0)

    def norm_mid():
        def one(i, _):
            rows = ds(i * RT, RT)
            mid = tokens[rows].astype(f32) + rms(total[rows]) * gains[1:2]
            after[rows] = mid
            act[0, ds(t * R + i * RT, RT)] = (rms(mid) * gains[2:3]).astype(bf16)
            return 0
        lax.fori_loop(0, R // RT, one, 0)

    def norm_out():
        def one(i, _):
            rows = ds(i * RT, RT)
            out[rows] = (after[rows] + rms(total[rows]) * gains[3:4]).astype(bf16)
            return 0
        lax.fori_loop(0, R // RT, one, 0)

    def tiles(width, tile, body):
        across = width // tile

        def one(i, _):
            body(ds((i // across) * TM, TM), ds((i % across) * tile, tile))
            return 0
        lax.fori_loop(0, (L // TM) * across, one, 0)

    def rotary(q, w, into, scale):
        def body(rows, cols):
            head = dot(act[q, rows], bufs[w][:, cols])
            lower, upper = head[:, :QK // 2], head[:, QK // 2:]
            cos, sin = cosine[rows], sine[rows]
            rotated = jnp.concatenate(
                [lower * cos - upper * sin, lower * sin + upper * cos], axis=-1)
            into[q, rows, cols] = (rotated * scale).astype(bf16)
        tiles(heads * QK, QK, body)

    def project_values(q):
        def body(rows, cols):
            values[q, rows, cols] = dot(act[q, rows], bufs[WV][:, cols]).astype(bf16)
        tiles(heads * VD, VD, body)

    def retain(q, h):
        head_index = (t * heads + h).astype(f32)
        fraction = jnp.full((1, 1), 1.0, f32) * (head_index / (heads * T - 1.0))
        log_decay = -(4.0 / BLOCK) * jnp.exp(fraction * math.log(BLOCK / (32.0 * L)))
        qk_cols = ds(h * QK, QK)
        v_cols = ds(h * VD, VD)
        for i in reversed(range(L // TM)):
            rows, seen = pl.ds(i * TM, TM), (i + 1) * TM
            scores = lax.dot_general(
                queries[q, rows, qk_cols], keys[q, :seen, qk_cols], (((1,), (1,)), ((), ())),
                preferred_element_type=f32)
            distance = (lax.broadcasted_iota(jnp.int32, (TM, seen), 0) + i * TM
                        - lax.broadcasted_iota(jnp.int32, (TM, seen), 1)).astype(f32)
            weights = jnp.where(
                distance >= 0, jnp.exp(log_decay * jnp.maximum(distance, 0.0)), 0.0)
            retained = dot((scores * weights).astype(bf16), values[q, :seen, v_cols])
            centred = retained - jnp.mean(retained, axis=-1, keepdims=True)
            normalized = centred * lax.rsqrt(
                jnp.mean(centred * centred, axis=-1, keepdims=True) + group_epsilon)
            swish = dot(act[q, rows], bufs[WS][:, v_cols])
            values[q, rows, v_cols] = (silu(swish) * normalized).astype(bf16)

    def retain_all(q):
        lax.fori_loop(0, heads, lambda h, _: (retain(q, h), 0)[1], 0)

    def hidden_units():
        def body(rows, cols):
            up = dot(act[0, rows], bufs[WU][:, cols])
            gate = dot(act[0, rows], bufs[WG][:, cols])
            values[0, rows, cols] = (silu(gate) * up).astype(bf16)
        tiles(FH, math.gcd(FH, 256), body)

    for w in range(8):
        local_copy(w).start()
    barrier = pltpu.get_barrier_semaphore()
    for condition, device in neighbours:
        when(condition, lambda device=device: pl.semaphore_signal(
            barrier, inc=1, device_id=device, device_id_type=MESH))
    fixed = (G - 1) + (X - 1) + 1
    pl.semaphore_wait(
        barrier, fixed + (f > 0).astype(jnp.int32) + (f < F - 1).astype(jnp.int32))

    comm(WQ, 0)
    norm_in()
    pl.when(is_end)(lambda: client_copy(host).start())
    pl.when(not_end)(lambda: gather_start(0))
    comm(WK, 0)
    for w in (WG, WU, WD):
        local_copy(w).wait()
        give_own(w, True)
    for k in range(1, F):
        comm(WQ, k)
    comm(WV, 0)
    comm(WK, 1)
    pl.when(not_end)(lambda: gather_forward(0))
    for k in range(2, F):
        comm(WK, k)
    comm(WS, 0)

    @pl.when(not_end)
    def _():
        gather_wait(0)
        arrived(WQ)
        rotary(0, WQ, queries, 1.0)
    comm(WV, 1)

    @pl.when(is_host)
    def _():
        client_copy(f).wait_recv()
        gather_start(1)

    @pl.when(not_end)
    def _():
        arrived(WK)
        rotary(0, WK, keys, QK ** -0.5)
    for k in range(2, F):
        comm(WV, k)
    comm(WM, 0)
    comm(WS, 1)

    @pl.when(not_end)
    def _():
        arrived(WV)
        project_values(0)
    pl.when(is_host)(lambda: gather_forward(1))
    comm(WG, 0)
    for k in range(2, F):
        comm(WS, k)

    @pl.when(is_host)
    def _():
        gather_wait(1)
        rotary(1, WQ, queries, 1.0)
        rotary(1, WK, keys, QK ** -0.5)
    comm(WM, 1)
    pl.when(is_host)(lambda: project_values(1))
    pl.when(not_end)(lambda: arrived(WS))
    if F > 2:
        comm(WM, 2)
    pl.when(is_host)(lambda: retain_all(1))
    for k in range(3, F):
        comm(WM, k)
    comm(WU, 0)
    pl.when(not_end)(lambda: retain_all(0))
    comm(WG, 1)
    pl.when(not_end)(lambda: gather_drain(0))

    slots = jnp.where(is_end, 0, jnp.where(is_host, 2, 1))

    def mixer(d, k):
        j = source(d, k)

        def one(n, _):
            q = slots - 1 - n
            sum_send(q, q, WM, heads * VD, j)
            return 0

        def two(n, _):
            q = slots - 1 - n
            sum_pass(q, q, WM, heads * VD, j)
            return 0
        lax.fori_loop(0, slots, one, 0)
        lax.fori_loop(0, slots, two, 0)

    mixer(0, 0)
    for k in range(1, F):
        for d in range(2):
            @pl.when(takes(WM, k, d))
            def _(k=k, d=d):
                arrived_from(WM, k, d)
                mixer(d, k)
    for k in range(2, F):
        comm(WG, k)
    comm(WD, 0)

    @pl.when(is_host)
    def _():
        def one(j, _):
            send1[1, j, 0] = sum_finish(1, 1, j).astype(bf16)
            give_back(j, outer).start()
            return 0
        lax.fori_loop(0, F, one, 0)

    @pl.when(not_end)
    def _():
        def one(j, _):
            acc[0, :, ds(j * cols, cols)] = sum_finish(0, 0, j)
            return 0
        lax.fori_loop(0, F, one, 0)
        sum_drain(0, 0)
    comm(WU, 1)

    @pl.when(is_end)
    def _():
        client_copy(host).wait_send()

        def one(j, _):
            give_back(j, f).wait_recv()
            acc[0, :, ds(j * cols, cols)] = recv2[0, j, 0].astype(f32)
            return 0
        lax.fori_loop(0, F, one, 0)
    norm_mid()
    gather_start(2)
    for k in range(2, F):
        comm(WU, k)
    comm(WD, 1)
    gather_forward(2)
    gather_wait(2)
    arrived(WG)
    arrived(WU)
    hidden_units()

    def down(j):
        sum_send(2, 0, WD, FH, j)
        sum_pass(2, 0, WD, FH, j)
    down(f)
    for k in range(1, F):
        if k > 1:
            comm(WD, k)
        for d in range(2):
            @pl.when(takes(WD, k, d))
            def _(k=k, d=d):
                arrived_from(WD, k, d)
                down(source(d, k))

    def finish(j, _):
        acc[0, :, ds(j * cols, cols)] = sum_finish(2, 0, j)
        return 0
    lax.fori_loop(0, F, finish, 0)
    norm_out()
    gather_drain(2)
    sum_drain(2, 0)

    @pl.when(is_host)
    def _():
        gather_drain(1)
        sum_drain(1, 1)

        def one(j, _):
            give_back(j, outer).wait_send()
            return 0
        lax.fori_loop(0, F, one, 0)
    for w in range(8):
        drain(w)


def per_device(tokens, norm_gains, *weights):
    G, F, T = lax.axis_size("grp"), lax.axis_size("fs"), lax.axis_size("tp")
    X = T // CORES
    R, D = tokens.shape
    L = R * T
    query, _, value, _, mixer, gate, _, down = weights
    qk_width, v_width, hidden = query.shape[1], value.shape[1], gate.shape[1]
    positions = jnp.arange(L, dtype=f32)
    frequency = 10000.0 ** (-jnp.linspace(0.0, 1.0, QK // 2, dtype=f32))
    angles = positions[:, None] * frequency[None, :]
    vmem = pl.BlockSpec(memory_space=pltpu.VMEM)
    anywhere = pl.BlockSpec(memory_space=pl.ANY)
    DMA = pltpu.SemaphoreType.DMA
    cols = mixer.shape[1]
    scratch = [pltpu.VMEM((w.shape[0] * F, w.shape[1]), bf16) for w in weights]
    scratch += [
        pltpu.VMEM((2, L, D), bf16),
        pltpu.VMEM((2, L, qk_width), bf16),
        pltpu.VMEM((2, L, qk_width), bf16),
        pltpu.VMEM((2, L, max(v_width, hidden)), bf16),
        pltpu.VMEM((2, R, D), f32),
        pltpu.VMEM((2, F, X, R, cols), bf16),
        pltpu.VMEM((2, F, X, R, cols), bf16),
        pltpu.VMEM((2, F, X, R, cols), bf16),
        DMA((8,)),
        DMA((2, 8, F)), DMA((2, 8, F)), DMA((2, 8, F, G)), DMA((2, 8, F, G)),
        DMA((8, G)), DMA((8, G)),
        DMA((3, X)), DMA((3, X)), DMA((3, X)), DMA((3, X)),
        DMA((3, F)), DMA((3, F)), DMA((3, F, X)), DMA((3, F, X)),
        DMA((2,)), DMA((F,)), DMA((F,)),
    ]
    return pl.pallas_call(
        functools.partial(layer, G, F, T),
        out_shape=jax.ShapeDtypeStruct((R, D), bf16),
        in_specs=[vmem] * 4 + [anywhere] * 8,
        out_specs=vmem,
        scratch_shapes=scratch,
        compiler_params=pltpu.CompilerParams(
            collective_id=0, has_side_effects=True, vmem_limit_bytes=67043328),
    )(tokens, norm_gains, jnp.cos(angles), jnp.sin(angles), *weights)


def solution(mesh):
    placed = (
        P(("grp", "fs", "tp"), None),
        P(),
        P("fs", "tp"),
        P("fs", "tp"),
        P("fs", "tp"),
        P("fs", "tp"),
        P("tp", "fs"),
        P("fs", "tp"),
        P("fs", "tp"),
        P("tp", "fs"),
    )
    return jax.shard_map(
        per_device,
        mesh=mesh,
        in_specs=placed,
        out_specs=P(("grp", "fs", "tp"), None),
        check_vma=False,
    )
```

```python
import functools
import math

import jax
import jax.numpy as jnp
from jax import lax
from jax.experimental import pallas as pl
from jax.experimental.pallas import tpu as pltpu
from jax.sharding import PartitionSpec as P

QK = 256
BLOCK = 128
CORES = 2

norm_epsilon = 1e-06
group_epsilon = 0.01

MESH = pl.DeviceIdType.MESH
f32, bf16 = jnp.float32, jnp.bfloat16

WQ, WK, WV, WS, WM, WG, WU, WD = range(8)


def rms(matrix):
    return matrix * lax.rsqrt(jnp.mean(matrix * matrix, axis=-1, keepdims=True) + norm_epsilon)


def silu(value):
    return value / (1.0 + jnp.exp(-value))


def dot(left, right):
    return jnp.dot(left, right, preferred_element_type=f32)


def ds(start, size, multiple=None):
    return pl.ds(pl.multiple_of(start, multiple or size), size)


MIXER = (WQ, WK, WV, WS, WM)
WHOLE = (WQ, WK, WV, WS, WG, WU, WD)


def layer(G, F, T, *refs):
    tokens, gains, cosine, sine = refs[:4]
    shards = refs[4:12]
    out = refs[12]
    bufs = refs[13:21]
    act, queries, keys, values, acc, send1, recv1, recv2 = refs[21:29]
    (local_sem, z_send, z_recv, y_send, y_recv, e_send, e_recv, ag_x_send, ag_x_recv, ag_c_send,
     ag_c_recv, rs1_send, rs1_recv, rs2_send, rs2_recv, client_sem, ret_send, ret_recv) = refs[29:]

    X = T // CORES
    g, f, t = lax.axis_index("grp"), lax.axis_index("fs"), lax.axis_index("tp")
    x, c = t // CORES, t % CORES
    R, D = tokens.shape
    L = R * T
    TM = min(256, L)
    heads = queries.shape[2] // QK
    VD = values.shape[2] // heads
    FH = bufs[WG].shape[1]
    total, after = acc.at[0], acc.at[1]
    partner = (g, f, x * CORES + (1 - c))

    moved = F >= 4
    is_end = (f == 0) | (f == F - 1) if moved else f < 0
    is_host = (f == 1) | (f == F - 2) if moved else f < 0
    not_end = jnp.logical_not(is_end)
    outer = jnp.where(f == 1, 0, F - 1)
    host = jnp.where(f == 0, 1, F - 2)

    def x_peer(o):
        return lax.rem(x + o, X)

    neighbours = [(f > 0, (g, f - 1, t)), (f < F - 1, (g, f + 1, t))]
    neighbours += [(None, (lax.rem(g + o, G), f, t)) for o in range(1, G)]
    neighbours += [(None, (g, f, x_peer(o) * CORES + c)) for o in range(1, X)]
    neighbours += [(None, partner)]

    def when(condition, action):
        if condition is None:
            action()
        else:
            pl.when(condition)(action)

    def local_copy(w):
        r = shards[w].shape[0]
        return pltpu.make_async_copy(shards[w], bufs[w].at[ds(f * r, r)], local_sem.at[w])

    def half(w, s, part):
        r = shards[w].shape[0]
        return bufs[w].at[ds(s * r + part * (r // G), r // G)]

    left = f * 2 < F
    ways = (jnp.where(left, 1, 0), jnp.where(left, 0, 1))
    steps = (2 * ways[0] - 1, 2 * ways[1] - 1)

    def source(d, k):
        return f + steps[d] * k

    def target(d):
        return f - steps[d]

    def valid(d, k):
        return (source(d, k) >= 0) & (source(d, k) < F)

    def has_next(w, d):
        margin = 1 if moved and w in MIXER else 0
        return (target(d) >= margin) & (target(d) <= F - 1 - margin)

    def takes(w, k, d):
        return valid(d, k) & not_end if w in MIXER else valid(d, k)

    def gives(w, k, d):
        return has_next(w, d) if k == 0 else takes(w, k, d) & has_next(w, d)

    def from_end(w, k, d):
        return is_host if w in WHOLE and k == 1 and d == 1 else None

    def crosses(w, k, d):
        special = from_end(w, k, d)
        if special is None:
            return takes(w, k, d)
        return takes(w, k, d) & jnp.logical_not(special)

    def z_copy(w, k, d):
        region = half(w, source(d, k), g)
        return pltpu.make_async_remote_copy(
            region, region, z_send.at[ways[d], w, k], z_recv.at[ways[d], w, k + 1],
            device_id=(g, target(d), t), device_id_type=MESH)

    def z_wait(w, k, d):
        region = half(w, source(d, k), g)
        pltpu.make_async_remote_copy(
            region, region, z_send.at[ways[d], w, k], z_recv.at[ways[d], w, k],
            device_id=(g, f, t), device_id_type=MESH).wait_recv()

    def y_copy(w, k, d, o):
        region = half(w, source(d, k), g)
        return pltpu.make_async_remote_copy(
            region, region, y_send.at[ways[d], w, k, o], y_recv.at[ways[d], w, k, o],
            device_id=(lax.rem(g + o, G), f, t), device_id_type=MESH)

    def y_wait(w, k, d, o):
        region = half(w, source(d, k), lax.rem(g + G - o, G))
        pltpu.make_async_remote_copy(
            region, region, y_send.at[ways[d], w, k, o], y_recv.at[ways[d], w, k, o],
            device_id=(g, f, t), device_id_type=MESH).wait_recv()

    def end_copy(w, o, s, device):
        region = half(w, s, lax.rem(g + o, G))
        return pltpu.make_async_remote_copy(
            region, region, e_send.at[w, o], e_recv.at[w, o],
            device_id=(g, device, t), device_id_type=MESH)

    def give_own(w, early):
        for d in range(2):
            if w in MIXER:
                condition = has_next(w, d)
            elif early:
                condition = is_host if d == 0 else None
            else:
                condition = has_next(w, d)
                if d == 0:
                    condition &= jnp.logical_not(is_host)
            if condition is not None:
                pl.when(condition)(lambda d=d: z_copy(w, 0, d).start())

    def give_rest(w):
        @pl.when(is_end)
        def _():
            for o in range(1, G):
                end_copy(w, o, f, host).start()

    def comm0(w):
        if w in MIXER:
            local_copy(w).wait()
        give_own(w, False)

    def pass_on(w, k, d, who=None):
        if k < F - 1:
            condition = gives(w, k, d)
            pl.when(condition if who is None else condition & who)(
                lambda: z_copy(w, k, d).start())

    def along_z(w, k, d, who=None, onward=True):
        pl.when(takes(w, k, d) if who is None else takes(w, k, d) & who)(
            lambda: z_wait(w, k, d))
        if onward:
            pass_on(w, k, d, who)

    def along_y(w, k, d, who=None):
        @pl.when(crosses(w, k, d) if who is None else crosses(w, k, d) & who)
        def _():
            for o in range(1, G):
                y_copy(w, k, d, o).start()

    def comm(w, k, d, who=None):
        along_z(w, k, d, who)
        along_y(w, k, d, who)

    reach = (range(1, F), range(1, (F - 1) // 2 + 1))

    def rest(w, d, who=None):
        for k in reach[d][1:]:
            comm(w, k, d, who)

    def arrived_from(w, k, d, who=None):
        def narrow(condition):
            return condition if who is None else condition & who

        @pl.when(narrow(crosses(w, k, d)))
        def _():
            for o in range(1, G):
                y_wait(w, k, d, o)
        special = from_end(w, k, d)
        if special is not None:
            @pl.when(narrow(special))
            def _():
                for o in range(1, G):
                    end_copy(w, o, source(d, k), f).wait_recv()

    def arrived(w):
        for d in range(2):
            for k in reach[d]:
                arrived_from(w, k, d)

    def drain(w):
        for d in range(2):
            for k in (0, *reach[d]):
                if k < F - 1:
                    pl.when(gives(w, k, d))(lambda k=k, d=d: z_copy(w, k, d).wait_send())
                if k > 0:
                    @pl.when(crosses(w, k, d))
                    def _(k=k, d=d):
                        for o in range(1, G):
                            y_copy(w, k, d, o).wait_send()
        if w in WHOLE:
            @pl.when(is_end)
            def _():
                for o in range(1, G):
                    end_copy(w, o, f, host).wait_send()

    def rows_of(q, device):
        return act.at[q, ds(device * R, R)]

    def slot(stage):
        return 1 if stage == 1 else 0

    def ag_x(stage, o):
        region = rows_of(slot(stage), t)
        return pltpu.make_async_remote_copy(
            region, region, ag_x_send.at[stage, o], ag_x_recv.at[stage, o],
            device_id=(g, f, x_peer(o) * CORES + c), device_id_type=MESH)

    def ag_c(stage, o, core):
        region = rows_of(slot(stage), x_peer(X - o) * CORES + core)
        return pltpu.make_async_remote_copy(
            region, region, ag_c_send.at[stage, o], ag_c_recv.at[stage, o],
            device_id=partner, device_id_type=MESH)

    def gather_start(stage):
        for o in range(1, X):
            ag_x(stage, o).start()
        ag_c(stage, 0, c).start()

    def gather_forward_one(stage, o):
        region = rows_of(slot(stage), x_peer(X - o) * CORES + c)
        pltpu.make_async_remote_copy(
            region, region, ag_x_send.at[stage, o], ag_x_recv.at[stage, o],
            device_id=(g, f, t), device_id_type=MESH).wait_recv()
        ag_c(stage, o, c).start()

    def gather_forward(stage):
        for o in range(1, X):
            gather_forward_one(stage, o)

    def gather_wait(stage):
        for o in range(X):
            ag_c(stage, o, 1 - c).wait_recv()

    def gather_drain(stage):
        for o in range(X):
            if o:
                ag_x(stage, o).wait_send()
            ag_c(stage, o, c).wait_send()

    def client_copy(device):
        return pltpu.make_async_remote_copy(
            rows_of(0, t), rows_of(1, t), client_sem.at[0], client_sem.at[1],
            device_id=(g, device, t), device_id_type=MESH)

    cols = send1.shape[-1]

    def rs1(stage, q, j):
        return pltpu.make_async_remote_copy(
            send1.at[q, j], recv1.at[q, j], rs1_send.at[stage, j], rs1_recv.at[stage, j],
            device_id=partner, device_id_type=MESH)

    def rs2(stage, q, j, o):
        return pltpu.make_async_remote_copy(
            send1.at[q, j, o], recv2.at[q, j, o], rs2_send.at[stage, j, o],
            rs2_recv.at[stage, j, o],
            device_id=(g, f, x_peer(o) * CORES + c), device_id_type=MESH)

    def give_back(j, device):
        return pltpu.make_async_remote_copy(
            send1.at[1, j, 0], recv2.at[0, j, 0], ret_send.at[j], ret_recv.at[j],
            device_id=(g, device, t), device_id_type=MESH)

    def partial_rows(w, width, q, j, device):
        r = shards[w].shape[0]
        return dot(values[q, ds(device * R, R), :width], bufs[w][ds(j * r, r), :])

    def sum_send(stage, q, w, width, j):
        def one(o, _):
            send1[q, j, o] = partial_rows(w, width, q, j, o * CORES + (1 - c)).astype(bf16)
            return 0
        lax.fori_loop(0, X, one, 0)
        rs1(stage, q, j).start()

    def sum_pass(stage, q, w, width, j):
        rs1(stage, q, j).wait()
        def pair(o):
            peer = x_peer(o)
            return (partial_rows(w, width, q, j, peer * CORES + c)
                    + recv1[q, j, peer].astype(f32))
        for o in range(1, X):
            send1[q, j, o] = pair(o).astype(bf16)
            rs2(stage, q, j, o).start()
        acc[q, :, ds(j * cols, cols)] = pair(0)

    def sum_finish(stage, q, j):
        block = acc[q, :, ds(j * cols, cols)]
        for o in range(1, X):
            rs2(stage, q, j, o).wait_recv()
            block += recv2[q, j, o].astype(f32)
        return block

    def sum_drain(stage, q):
        def one(j, _):
            for o in range(1, X):
                rs2(stage, q, j, o).wait_send()
            return 0
        lax.fori_loop(0, F, one, 0)

    RT = min(32, R)

    def norm_in():
        def one(i, _):
            rows = ds(i * RT, RT)
            act[0, ds(t * R + i * RT, RT)] = (
                rms(tokens[rows].astype(f32)) * gains[0:1]).astype(bf16)
            return 0
        lax.fori_loop(0, R // RT, one, 0)

    def norm_mid():
        def one(i, _):
            rows = ds(i * RT, RT)
            mid = tokens[rows].astype(f32) + rms(total[rows]) * gains[1:2]
            after[rows] = mid
            act[0, ds(t * R + i * RT, RT)] = (rms(mid) * gains[2:3]).astype(bf16)
            return 0
        lax.fori_loop(0, R // RT, one, 0)

    def norm_out():
        def one(i, _):
            rows = ds(i * RT, RT)
            out[rows] = (after[rows] + rms(total[rows]) * gains[3:4]).astype(bf16)
            return 0
        lax.fori_loop(0, R // RT, one, 0)

    def tiles(width, tile, body):
        across = width // tile

        def one(i, _):
            body(ds((i // across) * TM, TM), ds((i % across) * tile, tile))
            return 0
        lax.fori_loop(0, (L // TM) * across, one, 0)

    def rotary(q, w, into, scale):
        def body(rows, cols):
            head = dot(act[q, rows], bufs[w][:, cols])
            lower, upper = head[:, :QK // 2], head[:, QK // 2:]
            cos, sin = cosine[rows], sine[rows]
            rotated = jnp.concatenate(
                [lower * cos - upper * sin, lower * sin + upper * cos], axis=-1)
            into[q, rows, cols] = (rotated * scale).astype(bf16)
        tiles(heads * QK, QK, body)

    def project_values(q):
        def body(rows, cols):
            values[q, rows, cols] = dot(act[q, rows], bufs[WV][:, cols]).astype(bf16)
        tiles(heads * VD, VD, body)

    def retain(q, h):
        head_index = (t * heads + h).astype(f32)
        fraction = jnp.full((1, 1), 1.0, f32) * (head_index / (heads * T - 1.0))
        log_decay = -(4.0 / BLOCK) * jnp.exp(fraction * math.log(BLOCK / (32.0 * L)))
        qk_cols = ds(h * QK, QK)
        v_cols = ds(h * VD, VD)
        for i in reversed(range(L // TM)):
            rows, seen = pl.ds(i * TM, TM), (i + 1) * TM
            scores = lax.dot_general(
                queries[q, rows, qk_cols], keys[q, :seen, qk_cols], (((1,), (1,)), ((), ())),
                preferred_element_type=f32)
            distance = (lax.broadcasted_iota(jnp.int32, (TM, seen), 0) + i * TM
                        - lax.broadcasted_iota(jnp.int32, (TM, seen), 1)).astype(f32)
            weights = jnp.where(
                distance >= 0, jnp.exp(log_decay * jnp.maximum(distance, 0.0)), 0.0)
            retained = dot((scores * weights).astype(bf16), values[q, :seen, v_cols])
            centred = retained - jnp.mean(retained, axis=-1, keepdims=True)
            normalized = centred * lax.rsqrt(
                jnp.mean(centred * centred, axis=-1, keepdims=True) + group_epsilon)
            values[q, rows, v_cols] = normalized.astype(bf16)

    def retain_all(q):
        lax.fori_loop(0, heads, lambda h, _: (retain(q, h), 0)[1], 0)

    def project_swish(q):
        def body(rows, cols):
            swish = dot(act[q, rows], bufs[WS][:, cols])
            values[q, rows, cols] = (
                silu(swish) * values[q, rows, cols].astype(f32)).astype(bf16)
        tiles(heads * VD, VD, body)

    def hidden_units(device):
        tile = math.gcd(FH, 256)

        def one(i, _):
            rows, cols = ds(device * R, R), ds(i * tile, tile)
            up = dot(act[0, rows], bufs[WU][:, cols])
            gate = dot(act[0, rows], bufs[WG][:, cols])
            values[0, rows, cols] = (silu(gate) * up).astype(bf16)
            return 0
        lax.fori_loop(0, FH // tile, one, 0)

    def sums(stage, q, w, width, items, who=None, first=None):
        def condition(k, d):
            if k == 0:
                return who
            return takes(w, k, d) if who is None else takes(w, k, d) & who

        for n in range(len(items) + 1):
            if n < len(items):
                k, d = items[n]
                if k:
                    arrived_from(w, k, d, first)
                when(condition(k, d), lambda k=k, d=d: sum_send(stage, q, w, width, source(d, k)))
            if n > 0:
                k, d = items[n - 1]
                when(condition(k, d), lambda k=k, d=d: sum_pass(stage, q, w, width, source(d, k)))

    def finish_client(j):
        send1[1, j, 0] = sum_finish(1, 1, j).astype(bf16)
        give_back(j, outer).start()

    def finish_own(stage):
        def one(j, _):
            acc[0, :, ds(j * cols, cols)] = sum_finish(stage, 0, j)
            return 0
        lax.fori_loop(0, F, one, 0)

    def take_back():
        def one(j, _):
            give_back(j, f).wait_recv()
            acc[0, :, ds(j * cols, cols)] = recv2[0, j, 0].astype(f32)
            return 0
        lax.fori_loop(0, F, one, 0)

    far = [(k, d) for k in range(2, F) for d in range(2) if k in reach[d]]
    near = [(0, 0), (1, 0), (1, 1)]
    guest = not_end & jnp.logical_not(is_host)

    for w in range(8):
        local_copy(w).start()
    barrier = pltpu.get_barrier_semaphore()
    for condition, device in neighbours:
        when(condition, lambda device=device: pl.semaphore_signal(
            barrier, inc=1, device_id=device, device_id_type=MESH))
    fixed = (G - 1) + (X - 1) + 1
    pl.semaphore_wait(
        barrier, fixed + (f > 0).astype(jnp.int32) + (f < F - 1).astype(jnp.int32))

    comm0(WQ)
    give_rest(WQ)
    norm_in()
    pl.when(is_end)(lambda: client_copy(host).start())
    pl.when(not_end)(lambda: gather_start(0))
    comm0(WK)
    for w in (WG, WU, WD):
        local_copy(w).wait()
        give_own(w, True)
    comm(WQ, 1, 0)
    comm(WQ, 1, 1)
    rest(WQ, 0)
    rest(WQ, 1)
    comm0(WV)
    comm(WK, 1, 0)

    @pl.when(not_end)
    def _():
        gather_forward(0)
        gather_wait(0)
        arrived(WQ)
        rotary(0, WQ, queries, 1.0)
    comm(WV, 1, 0)
    give_rest(WK)
    comm0(WS)
    give_rest(WV)
    give_rest(WS)

    @pl.when(is_host)
    def _():
        client_copy(f).wait_recv()
        gather_start(1)
    comm(WK, 1, 1)
    rest(WK, 0)
    rest(WK, 1)
    comm(WS, 1, 0)
    comm(WV, 1, 1)
    comm0(WM)

    @pl.when(is_end)
    def _():
        for w in (WG, WU, WD):
            give_own(w, False)
        for w in (WG, WU, WD):
            give_rest(w)

    @pl.when(not_end)
    def _():
        arrived(WK)
        rotary(0, WK, keys, QK ** -0.5)

    @pl.when(is_host)
    def _():
        gather_forward(1)
        gather_wait(1)
        rotary(1, WQ, queries, 1.0)
    rest(WV, 0)
    rest(WV, 1)
    comm(WS, 1, 1)
    pl.when(is_host)(lambda: rotary(1, WK, keys, QK ** -0.5))
    pl.when(not_end)(lambda: arrived(WV))
    pl.when(is_host)(lambda: project_values(1))
    rest(WS, 0)
    rest(WS, 1)

    @pl.when(not_end)
    def _():
        give_own(WG, False)
        give_own(WU, False)
        give_own(WD, False)
    comm(WM, 1, 0)
    pl.when(is_host)(lambda: retain_all(1))
    pl.when(not_end)(lambda: project_values(0))
    along_z(WG, 1, 0)
    along_y(WG, 1, 0, is_end)
    pl.when(not_end)(lambda: retain_all(0))
    pl.when(not_end)(lambda: arrived(WS))
    pl.when(is_host)(lambda: project_swish(1))
    comm(WM, 1, 1)
    along_z(WU, 1, 0)
    along_y(WU, 1, 0, is_end)
    sums(1, 1, WM, heads * VD, near[:2], is_host, is_host)
    comm(WG, 1, 1)
    along_z(WD, 1, 0)
    along_y(WD, 1, 0, is_end)
    pl.when(not_end)(lambda: project_swish(0))
    along_y(WG, 1, 0, not_end)
    pl.when(not_end)(lambda: gather_drain(0))

    @pl.when(is_host)
    def _():
        finish_client(f)
        finish_client(source(0, 1))
    sums(0, 0, WM, heads * VD, near[:1], not_end, guest)
    comm(WU, 1, 1)
    rest(WM, 0)
    rest(WM, 1)
    sums(1, 1, WM, heads * VD, near[2:], is_host, is_host)
    along_y(WU, 1, 0, not_end)
    sums(0, 0, WM, heads * VD, near[1:2], not_end, guest)
    rest(WG, 0, not_end)
    rest(WG, 1)
    comm(WD, 1, 1)
    sums(1, 1, WM, heads * VD, far, is_host, is_host)
    sums(0, 0, WM, heads * VD, near[2:] + far, not_end, guest)
    pl.when(is_host)(lambda: finish_client(source(1, 1)))
    for k in range(2, F):
        along_z(WU, k, 0, not_end, False)
        along_y(WU, k, 0, not_end)
    rest(WU, 1)
    along_y(WD, 1, 0, not_end)
    for k, d in far:
        pl.when(takes(WM, k, d) & is_host)(lambda k=k, d=d: finish_client(source(d, k)))
    for k in range(2, F):
        pass_on(WU, k, 0, not_end)
    rest(WD, 0, not_end)
    rest(WD, 1)
    for w in (WG, WU, WD):
        comm(w, 2, 0, is_end)
    for k in range(3, F):
        comm(WG, k, 0, is_end)

    @pl.when(is_end)
    def _():
        client_copy(host).wait_send()
        take_back()
        norm_mid()
        gather_start(2)

    @pl.when(not_end)
    def _():
        finish_own(0)
        sum_drain(0, 0)
        norm_mid()
        gather_start(2)
    for k in range(3, F):
        comm(WU, k, 0, is_end)
        comm(WD, k, 0, is_end)
    arrived(WG)
    arrived(WU)
    ag_c(2, 0, 1 - c).wait_recv()
    hidden_units(t)
    hidden_units(x * CORES + 1 - c)
    for o in range(1, X):
        gather_forward_one(2, o)
        hidden_units(x_peer(X - o) * CORES + c)
    for o in range(1, X):
        ag_c(2, o, 1 - c).wait_recv()
        hidden_units(x_peer(X - o) * CORES + 1 - c)
    sums(2, 0, WD, FH, near)
    for k, d in far:
        sums(2, 0, WD, FH, [(k, d)])
    finish_own(2)
    norm_out()
    gather_drain(2)
    sum_drain(2, 0)

    @pl.when(is_host)
    def _():
        gather_drain(1)
        sum_drain(1, 1)

        def one(j, _):
            give_back(j, outer).wait_send()
            return 0
        lax.fori_loop(0, F, one, 0)
    for w in range(8):
        drain(w)


def per_device(tokens, norm_gains, *weights):
    G, F, T = lax.axis_size("grp"), lax.axis_size("fs"), lax.axis_size("tp")
    X = T // CORES
    R, D = tokens.shape
    L = R * T
    query, _, value, _, mixer, gate, _, down = weights
    qk_width, v_width, hidden = query.shape[1], value.shape[1], gate.shape[1]
    positions = jnp.arange(L, dtype=f32)
    frequency = 10000.0 ** (-jnp.linspace(0.0, 1.0, QK // 2, dtype=f32))
    angles = positions[:, None] * frequency[None, :]
    vmem = pl.BlockSpec(memory_space=pltpu.VMEM)
    anywhere = pl.BlockSpec(memory_space=pl.ANY)
    DMA = pltpu.SemaphoreType.DMA
    cols = mixer.shape[1]
    scratch = [pltpu.VMEM((w.shape[0] * F, w.shape[1]), bf16) for w in weights]
    scratch += [
        pltpu.VMEM((2, L, D), bf16),
        pltpu.VMEM((2, L, qk_width), bf16),
        pltpu.VMEM((2, L, qk_width), bf16),
        pltpu.VMEM((2, L, max(v_width, hidden)), bf16),
        pltpu.VMEM((2, R, D), f32),
        pltpu.VMEM((2, F, X, R, cols), bf16),
        pltpu.VMEM((2, F, X, R, cols), bf16),
        pltpu.VMEM((2, F, X, R, cols), bf16),
        DMA((8,)),
        DMA((2, 8, F)), DMA((2, 8, F)), DMA((2, 8, F, G)), DMA((2, 8, F, G)),
        DMA((8, G)), DMA((8, G)),
        DMA((3, X)), DMA((3, X)), DMA((3, X)), DMA((3, X)),
        DMA((3, F)), DMA((3, F)), DMA((3, F, X)), DMA((3, F, X)),
        DMA((2,)), DMA((F,)), DMA((F,)),
    ]
    return pl.pallas_call(
        functools.partial(layer, G, F, T),
        out_shape=jax.ShapeDtypeStruct((R, D), bf16),
        in_specs=[vmem] * 4 + [anywhere] * 8,
        out_specs=vmem,
        scratch_shapes=scratch,
        compiler_params=pltpu.CompilerParams(
            collective_id=0, has_side_effects=True, vmem_limit_bytes=67043328),
    )(tokens, norm_gains, jnp.cos(angles), jnp.sin(angles), *weights)


def solution(mesh):
    placed = (
        P(("grp", "fs", "tp"), None),
        P(),
        P("fs", "tp"),
        P("fs", "tp"),
        P("fs", "tp"),
        P("fs", "tp"),
        P("tp", "fs"),
        P("fs", "tp"),
        P("fs", "tp"),
        P("tp", "fs"),
    )
    return jax.shard_map(
        per_device,
        mesh=mesh,
        in_specs=placed,
        out_specs=P(("grp", "fs", "tp"), None),
        check_vma=False,
    )
```

```python
import functools
import math

import jax
import jax.numpy as jnp
import numpy as np
from jax import lax
from jax.experimental import pallas as pl
from jax.experimental.pallas import tpu as pltpu
from jax.sharding import PartitionSpec as P

QK = 256
BLOCK = 128
CORES = 2

norm_epsilon = 1e-06
group_epsilon = 0.01

MESH = pl.DeviceIdType.MESH
f32, bf16 = jnp.float32, jnp.bfloat16

WQ, WK, WV, WS, WM, WG, WU, WD = range(8)


def rms(matrix):
    return matrix * lax.rsqrt(jnp.mean(matrix * matrix, axis=-1, keepdims=True) + norm_epsilon)


def silu(value):
    return value / (1.0 + jnp.exp(-value))


def dot(left, right):
    return jnp.dot(left, right, preferred_element_type=f32)


def ds(start, size, multiple=None):
    return pl.ds(pl.multiple_of(start, multiple or size), size)


MIXER = (WQ, WK, WV, WS, WM)
WHOLE = (WQ, WK, WV, WS, WG, WU, WD)


def layer(G, F, T, *refs):
    tokens, gains, coarse, fine = refs[:4]
    shards = refs[4:12]
    out = refs[12]
    bufs = refs[13:21]
    act, queries, keys, values, acc, send1, recv1, recv2 = refs[21:29]
    cosine, sine, rows_out = refs[29:32]
    (local_sem, z_send, z_recv, y_send, y_recv, e_send, e_recv, ag_x_send, ag_x_recv, ag_c_send,
     ag_c_recv, rs1_send, rs1_recv, rs2_send, rs2_recv, client_sem, ret_send, ret_recv, out_sem) = refs[32:]

    X = T // CORES
    g, f, t = lax.axis_index("grp"), lax.axis_index("fs"), lax.axis_index("tp")
    x, c = t // CORES, t % CORES
    R, D = tokens.shape
    L = R * T
    TM = min(256, L)
    heads = queries.shape[2] // QK
    VD = values.shape[2] // heads
    FH = bufs[WG].shape[1]
    total, after = acc.at[0], acc.at[1]
    partner = (g, f, x * CORES + (1 - c))

    moved = F >= 4
    is_end = (f == 0) | (f == F - 1) if moved else f < 0
    is_host = (f == 1) | (f == F - 2) if moved else f < 0
    not_end = jnp.logical_not(is_end)
    outer = jnp.where(f == 1, 0, F - 1)
    host = jnp.where(f == 0, 1, F - 2)

    def x_peer(o):
        return lax.rem(x + o, X)

    neighbours = [(f > 0, (g, f - 1, t)), (f < F - 1, (g, f + 1, t))]
    neighbours += [(None, (lax.rem(g + o, G), f, t)) for o in range(1, G)]
    neighbours += [(None, (g, f, x_peer(o) * CORES + c)) for o in range(1, X)]
    neighbours += [(None, partner)]

    def when(condition, action):
        if condition is None:
            action()
        else:
            pl.when(condition)(action)

    def local_copy(w):
        r = shards[w].shape[0]
        return pltpu.make_async_copy(shards[w], bufs[w].at[ds(f * r, r)], local_sem.at[w])

    def half(w, s, part):
        r = shards[w].shape[0]
        return bufs[w].at[ds(s * r + part * (r // G), r // G)]

    left = f * 2 < F
    ways = (jnp.where(left, 1, 0), jnp.where(left, 0, 1))
    steps = (2 * ways[0] - 1, 2 * ways[1] - 1)

    def source(d, k):
        return f + steps[d] * k

    def target(d):
        return f - steps[d]

    def valid(d, k):
        return (source(d, k) >= 0) & (source(d, k) < F)

    def has_next(w, d):
        margin = 1 if moved and w in MIXER else 0
        return (target(d) >= margin) & (target(d) <= F - 1 - margin)

    def takes(w, k, d):
        return valid(d, k) & not_end if w in MIXER else valid(d, k)

    def gives(w, k, d):
        return has_next(w, d) if k == 0 else takes(w, k, d) & has_next(w, d)

    def from_end(w, k, d):
        return is_host if w in WHOLE and k == 1 and d == 1 else None

    def crosses(w, k, d):
        special = from_end(w, k, d)
        if special is None:
            return takes(w, k, d)
        return takes(w, k, d) & jnp.logical_not(special)

    def z_place(d, k):
        return k if d == 0 else F - 1 + k

    def y_place(d, k):
        return k - 1 if d == 0 else F - 2 + k

    def z_copy(w, k, d):
        region = half(w, source(d, k), g)
        return pltpu.make_async_remote_copy(
            region, region, z_send.at[w, z_place(d, k)], z_recv.at[w, source(d, k)],
            device_id=(g, target(d), t), device_id_type=MESH)

    def z_wait(w, k, d):
        region = half(w, source(d, k), g)
        pltpu.make_async_remote_copy(
            region, region, z_send.at[w, 0], z_recv.at[w, source(d, k)],
            device_id=(g, f, t), device_id_type=MESH).wait_recv()

    def y_copy(w, k, d, o):
        region = half(w, source(d, k), g)
        return pltpu.make_async_remote_copy(
            region, region, y_send.at[w, y_place(d, k), o - 1], y_recv.at[w, y_place(d, k), o - 1],
            device_id=(lax.rem(g + o, G), f, t), device_id_type=MESH)

    def y_wait(w, k, d, o):
        region = half(w, source(d, k), lax.rem(g + G - o, G))
        pltpu.make_async_remote_copy(
            region, region, y_send.at[w, y_place(d, k), o - 1], y_recv.at[w, y_place(d, k), o - 1],
            device_id=(g, f, t), device_id_type=MESH).wait_recv()

    def end_copy(w, o, s, device):
        region = half(w, s, lax.rem(g + o, G))
        return pltpu.make_async_remote_copy(
            region, region, e_send.at[w, o - 1], e_recv.at[w, o - 1],
            device_id=(g, device, t), device_id_type=MESH)

    def give_own(w, early):
        for d in range(2):
            if w in MIXER:
                condition = has_next(w, d)
            elif early:
                condition = is_host if d == 0 else None
            else:
                condition = has_next(w, d)
                if d == 0:
                    condition &= jnp.logical_not(is_host)
            if condition is not None:
                pl.when(condition)(lambda d=d: z_copy(w, 0, d).start())

    def give_rest(w):
        @pl.when(is_end)
        def _():
            for o in range(1, G):
                end_copy(w, o, f, host).start()

    def comm0(w):
        if w in MIXER:
            local_copy(w).wait()
        give_own(w, False)

    def pass_on(w, k, d, who=None):
        if k < F - 1:
            condition = gives(w, k, d)
            pl.when(condition if who is None else condition & who)(
                lambda: z_copy(w, k, d).start())

    def along_z(w, k, d, who=None, onward=True):
        pl.when(takes(w, k, d) if who is None else takes(w, k, d) & who)(
            lambda: z_wait(w, k, d))
        if onward:
            pass_on(w, k, d, who)

    def along_y(w, k, d, who=None):
        @pl.when(crosses(w, k, d) if who is None else crosses(w, k, d) & who)
        def _():
            for o in range(1, G):
                y_copy(w, k, d, o).start()

    def comm(w, k, d, who=None):
        along_z(w, k, d, who)
        along_y(w, k, d, who)

    reach = (range(1, F), range(1, (F - 1) // 2 + 1))

    def rest(w, d, who=None):
        for k in reach[d][1:]:
            comm(w, k, d, who)

    def arrived_from(w, k, d, who=None):
        def narrow(condition):
            return condition if who is None else condition & who

        @pl.when(narrow(crosses(w, k, d)))
        def _():
            for o in range(1, G):
                y_wait(w, k, d, o)
        special = from_end(w, k, d)
        if special is not None:
            @pl.when(narrow(special))
            def _():
                for o in range(1, G):
                    end_copy(w, o, source(d, k), f).wait_recv()

    def arrived(w):
        for d in range(2):
            for k in reach[d]:
                arrived_from(w, k, d)

    def drain(w):
        for d in range(2):
            for k in (0, *reach[d]):
                if k < F - 1:
                    pl.when(gives(w, k, d))(lambda k=k, d=d: z_copy(w, k, d).wait_send())
                if k > 0:
                    @pl.when(crosses(w, k, d))
                    def _(k=k, d=d):
                        for o in range(1, G):
                            y_copy(w, k, d, o).wait_send()
        if w in WHOLE:
            @pl.when(is_end)
            def _():
                for o in range(1, G):
                    end_copy(w, o, f, host).wait_send()

    def rows_of(q, device):
        return act.at[q, ds(device * R, R)]

    def slot(stage):
        return 1 if stage == 1 else 0

    HALF = R // 2

    def window(stage):
        return ds((stage - 2) * HALF, HALF) if stage > 1 else ds(0, R)

    def block_of(stage, device):
        if stage > 1:
            return act.at[0, ds(device * R + (stage - 2) * HALF, HALF)]
        return rows_of(slot(stage), device)

    def ag_x(stage, o):
        region = block_of(stage, t)
        return pltpu.make_async_remote_copy(
            region, region, ag_x_send.at[stage, o - 1], ag_x_recv.at[stage, o - 1],
            device_id=(g, f, x_peer(o) * CORES + c), device_id_type=MESH)

    def ag_c(stage, o, core):
        region = block_of(stage, x_peer(X - o) * CORES + core)
        return pltpu.make_async_remote_copy(
            region, region, ag_c_send.at[stage, o], ag_c_recv.at[stage, o],
            device_id=partner, device_id_type=MESH)

    def gather_start(stage):
        for o in range(1, X):
            ag_x(stage, o).start()
        ag_c(stage, 0, c).start()

    def gather_forward_one(stage, o):
        region = block_of(stage, x_peer(X - o) * CORES + c)
        pltpu.make_async_remote_copy(
            region, region, ag_x_send.at[stage, o - 1], ag_x_recv.at[stage, o - 1],
            device_id=(g, f, t), device_id_type=MESH).wait_recv()
        ag_c(stage, o, c).start()

    def gather_forward(stage):
        for o in range(1, X):
            gather_forward_one(stage, o)

    def gather_wait(stage):
        for o in range(X):
            ag_c(stage, o, 1 - c).wait_recv()

    def gather_drain(stage):
        for o in range(X):
            if o:
                ag_x(stage, o).wait_send()
            ag_c(stage, o, c).wait_send()

    def client_copy(device):
        return pltpu.make_async_remote_copy(
            rows_of(0, t), rows_of(1, t), client_sem.at[0], client_sem.at[1],
            device_id=(g, device, t), device_id_type=MESH)

    cols = send1.shape[-1]

    def rs1(stage, q, j):
        return pltpu.make_async_remote_copy(
            send1.at[q, j, :, window(stage)], recv1.at[q, j, :, window(stage)],
            rs1_send.at[stage, j], rs1_recv.at[stage, j],
            device_id=partner, device_id_type=MESH)

    def rs2(stage, q, j, o):
        return pltpu.make_async_remote_copy(
            send1.at[q, j, o, window(stage)], recv2.at[q, j, o, window(stage)],
            rs2_send.at[stage, j, o - 1], rs2_recv.at[stage, j, o - 1],
            device_id=(g, f, x_peer(o) * CORES + c), device_id_type=MESH)

    def give_back(j, device):
        return pltpu.make_async_remote_copy(
            send1.at[1, j, 0], recv2.at[0, j, 0], ret_send.at[j], ret_recv.at[j],
            device_id=(g, device, t), device_id_type=MESH)

    def partial_rows(stage, w, width, q, j, device):
        r = shards[w].shape[0]
        rows = (ds(device * R + (stage - 2) * HALF, HALF) if stage > 1 else ds(device * R, R))
        return dot(values[q, rows, :width], bufs[w][ds(j * r, r), :])

    def sum_send(stage, q, w, width, j):
        def one(o, _):
            send1[q, j, o, window(stage)] = partial_rows(
                stage, w, width, q, j, o * CORES + (1 - c)).astype(bf16)
            return 0
        lax.fori_loop(0, X, one, 0)
        rs1(stage, q, j).start()

    def sum_pass(stage, q, w, width, j):
        rs1(stage, q, j).wait()
        def pair(o):
            peer = x_peer(o)
            return (partial_rows(stage, w, width, q, j, peer * CORES + c)
                    + recv1[q, j, peer, window(stage)].astype(f32))
        for o in range(1, X):
            send1[q, j, o, window(stage)] = pair(o).astype(bf16)
            rs2(stage, q, j, o).start()
        acc[q, window(stage), ds(j * cols, cols)] = pair(0)

    def sum_finish(stage, q, j):
        block = acc[q, window(stage), ds(j * cols, cols)]
        for o in range(1, X):
            rs2(stage, q, j, o).wait_recv()
            block += recv2[q, j, o, window(stage)].astype(f32)
        return block

    def sum_drain(stage, q):
        def one(j, _):
            for o in range(1, X):
                rs2(stage, q, j, o).wait_send()
            return 0
        lax.fori_loop(0, F, one, 0)

    RT = min(32, R // 2)

    def norm_in():
        def one(i, _):
            rows = ds(i * RT, RT)
            act[0, ds(t * R + i * RT, RT)] = (
                rms(tokens[rows].astype(f32)) * gains[0:1]).astype(bf16)
            return 0
        lax.fori_loop(0, R // RT, one, 0)

    def norm_mid(part):
        def one(i, _):
            rows = ds(i * RT, RT)
            mid = tokens[rows].astype(f32) + rms(total[rows]) * gains[1:2]
            after[rows] = mid
            act[0, ds(t * R + i * RT, RT)] = (rms(mid) * gains[2:3]).astype(bf16)
            return 0
        count = HALF // RT
        lax.fori_loop(part * count, (part + 1) * count, one, 0)

    PARTS = 4

    def out_copy(part):
        rows = ds(part * (R // PARTS), R // PARTS)
        return pltpu.make_async_copy(rows_out.at[rows], out.at[rows], out_sem.at[part])

    def norm_out(half):
        tall = min(RT, R // PARTS)

        def one(i, _):
            rows = ds(i * tall, tall)
            rows_out[rows] = (after[rows] + rms(total[rows]) * gains[3:4]).astype(bf16)
            return 0
        count = R // PARTS // tall
        for part in range(half * PARTS // 2, (half + 1) * PARTS // 2):
            lax.fori_loop(part * count, (part + 1) * count, one, 0)
            out_copy(part).start()

    def tables():
        step = fine.shape[1]

        def one(i, _):
            rows = ds(i * step, step)
            far_cos, far_sin = coarse[0, pl.ds(i, 1)], coarse[1, pl.ds(i, 1)]
            cosine[rows] = far_cos * fine[0] - far_sin * fine[1]
            sine[rows] = far_sin * fine[0] + far_cos * fine[1]
            return 0
        lax.fori_loop(0, L // step, one, 0)

    def tiles(width, tile, body):
        across = width // tile

        def one(i, _):
            body(ds((i // across) * TM, TM), ds((i % across) * tile, tile))
            return 0
        lax.fori_loop(0, (L // TM) * across, one, 0)

    def rotary(q, w, into, scale):
        def body(rows, cols):
            head = dot(act[q, rows], bufs[w][:, cols])
            lower, upper = head[:, :QK // 2], head[:, QK // 2:]
            cos, sin = cosine[rows], sine[rows]
            rotated = jnp.concatenate(
                [lower * cos - upper * sin, lower * sin + upper * cos], axis=-1)
            into[q, rows, cols] = (rotated * scale).astype(bf16)
        tiles(heads * QK, QK, body)

    def project_values(q):
        def body(rows, cols):
            values[q, rows, cols] = dot(act[q, rows], bufs[WV][:, cols]).astype(bf16)
        tiles(heads * VD, VD, body)

    def retain(q, h):
        head_index = (t * heads + h).astype(f32)
        fraction = jnp.full((1, 1), 1.0, f32) * (head_index / (heads * T - 1.0))
        log_decay = -(4.0 / BLOCK) * jnp.exp(fraction * math.log(BLOCK / (32.0 * L)))
        qk_cols = ds(h * QK, QK)
        v_cols = ds(h * VD, VD)
        for i in reversed(range(L // TM)):
            rows, seen = pl.ds(i * TM, TM), (i + 1) * TM
            scores = lax.dot_general(
                queries[q, rows, qk_cols], keys[q, :seen, qk_cols], (((1,), (1,)), ((), ())),
                preferred_element_type=f32)
            distance = (lax.broadcasted_iota(jnp.int32, (TM, seen), 0) + i * TM
                        - lax.broadcasted_iota(jnp.int32, (TM, seen), 1)).astype(f32)
            weights = jnp.where(
                distance >= 0, jnp.exp(log_decay * jnp.maximum(distance, 0.0)), 0.0)
            retained = dot((scores * weights).astype(bf16), values[q, :seen, v_cols])
            centred = retained - jnp.mean(retained, axis=-1, keepdims=True)
            normalized = centred * lax.rsqrt(
                jnp.mean(centred * centred, axis=-1, keepdims=True) + group_epsilon)
            values[q, rows, v_cols] = normalized.astype(bf16)

    def retain_all(q):
        lax.fori_loop(0, heads, lambda h, _: (retain(q, h), 0)[1], 0)

    def project_swish(q):
        def body(rows, cols):
            swish = dot(act[q, rows], bufs[WS][:, cols])
            values[q, rows, cols] = (
                silu(swish) * values[q, rows, cols].astype(f32)).astype(bf16)
        tiles(heads * VD, VD, body)

    def hidden_units(device, part):
        tile = math.gcd(FH, 256)

        def one(i, _):
            rows, cols = ds(device * R + part * HALF, HALF), ds(i * tile, tile)
            up = dot(act[0, rows], bufs[WU][:, cols])
            gate = dot(act[0, rows], bufs[WG][:, cols])
            values[0, rows, cols] = (silu(gate) * up).astype(bf16)
            return 0
        lax.fori_loop(0, FH // tile, one, 0)

    def sums(stage, q, w, width, items, who=None, first=None, wait=True):
        def condition(k, d):
            if k == 0:
                return who
            return takes(w, k, d) if who is None else takes(w, k, d) & who

        for n in range(len(items) + 1):
            if n < len(items):
                k, d = items[n]
                if k and wait:
                    arrived_from(w, k, d, first)
                when(condition(k, d), lambda k=k, d=d: sum_send(stage, q, w, width, source(d, k)))
            if n > 0:
                k, d = items[n - 1]
                when(condition(k, d), lambda k=k, d=d: sum_pass(stage, q, w, width, source(d, k)))

    def finish_client(j):
        send1[1, j, 0] = sum_finish(1, 1, j).astype(bf16)
        give_back(j, outer).start()

    def finish_own(stage):
        def one(j, _):
            acc[0, window(stage), ds(j * cols, cols)] = sum_finish(stage, 0, j)
            return 0
        lax.fori_loop(0, F, one, 0)

    def take_back():
        def one(j, _):
            give_back(j, f).wait_recv()
            acc[0, :, ds(j * cols, cols)] = recv2[0, j, 0].astype(f32)
            return 0
        lax.fori_loop(0, F, one, 0)

    far = [(k, d) for k in range(2, F) for d in range(2) if k in reach[d]]
    near = [(0, 0), (1, 0), (1, 1)]
    guest = not_end & jnp.logical_not(is_host)

    for w in range(8):
        local_copy(w).start()
    barrier = pltpu.get_barrier_semaphore()
    for condition, device in neighbours:
        when(condition, lambda device=device: pl.semaphore_signal(
            barrier, inc=1, device_id=device, device_id_type=MESH))
    fixed = (G - 1) + (X - 1) + 1
    pl.semaphore_wait(
        barrier, fixed + (f > 0).astype(jnp.int32) + (f < F - 1).astype(jnp.int32))

    comm0(WQ)
    give_rest(WQ)
    norm_in()
    pl.when(is_end)(lambda: client_copy(host).start())
    pl.when(not_end)(lambda: gather_start(0))
    comm0(WK)
    for w in (WG, WU, WD):
        local_copy(w).wait()
        give_own(w, True)
    pl.when(not_end)(tables)
    comm(WQ, 1, 0)
    comm(WQ, 1, 1)
    rest(WQ, 0)
    rest(WQ, 1)
    comm0(WV)
    comm(WK, 1, 0)

    @pl.when(not_end)
    def _():
        gather_forward(0)
        gather_wait(0)
        arrived(WQ)
        rotary(0, WQ, queries, 1.0)
    comm(WV, 1, 0)
    give_rest(WK)
    comm0(WS)
    give_rest(WV)
    give_rest(WS)

    @pl.when(is_host)
    def _():
        client_copy(f).wait_recv()
        gather_start(1)
    comm(WK, 1, 1)
    rest(WK, 0)
    rest(WK, 1)
    comm(WS, 1, 0)
    comm(WV, 1, 1)
    comm0(WM)

    @pl.when(is_end)
    def _():
        for w in (WG, WU, WD):
            give_own(w, False)
        for w in (WG, WU, WD):
            give_rest(w)

    @pl.when(not_end)
    def _():
        arrived(WK)
        rotary(0, WK, keys, QK ** -0.5)

    @pl.when(is_host)
    def _():
        gather_forward(1)
        gather_wait(1)
        rotary(1, WQ, queries, 1.0)
    rest(WV, 0)
    rest(WV, 1)
    comm(WS, 1, 1)
    pl.when(is_host)(lambda: rotary(1, WK, keys, QK ** -0.5))
    pl.when(not_end)(lambda: arrived(WV))
    pl.when(is_host)(lambda: project_values(1))
    rest(WS, 0)
    rest(WS, 1)

    @pl.when(not_end)
    def _():
        give_own(WG, False)
        give_own(WU, False)
        give_own(WD, False)
    comm(WM, 1, 0)
    pl.when(is_host)(lambda: retain_all(1))
    pl.when(not_end)(lambda: project_values(0))
    along_z(WG, 1, 0)
    along_y(WG, 1, 0, is_end)
    pl.when(not_end)(lambda: retain_all(0))
    pl.when(not_end)(lambda: arrived(WS))
    pl.when(is_host)(lambda: project_swish(1))
    comm(WM, 1, 1)
    along_z(WU, 1, 0)
    along_y(WU, 1, 0, is_end)
    sums(1, 1, WM, heads * VD, near[:2], is_host, is_host)
    comm(WG, 1, 1)
    along_z(WD, 1, 0)
    along_y(WD, 1, 0, is_end)
    pl.when(not_end)(lambda: project_swish(0))
    along_y(WG, 1, 0, not_end)
    pl.when(not_end)(lambda: gather_drain(0))

    @pl.when(is_host)
    def _():
        finish_client(f)
        finish_client(source(0, 1))
    sums(0, 0, WM, heads * VD, near[:1], not_end, guest)
    comm(WU, 1, 1)
    rest(WM, 0)
    rest(WM, 1)
    sums(1, 1, WM, heads * VD, near[2:], is_host, is_host)
    along_y(WU, 1, 0, not_end)
    sums(0, 0, WM, heads * VD, near[1:2], not_end, guest)
    rest(WG, 0, not_end)
    rest(WG, 1)
    comm(WD, 1, 1)
    sums(1, 1, WM, heads * VD, far, is_host, is_host)
    pl.when(is_host)(lambda: finish_client(source(1, 1)))
    sums(0, 0, WM, heads * VD, near[2:] + far, not_end, guest)
    for k in range(2, F):
        along_z(WU, k, 0, not_end, False)
        along_y(WU, k, 0, not_end)
    rest(WU, 1)
    along_y(WD, 1, 0, not_end)
    for k, d in far:
        pl.when(takes(WM, k, d) & is_host)(lambda k=k, d=d: finish_client(source(d, k)))
    for k in range(2, F):
        pass_on(WU, k, 0, not_end)
    rest(WD, 0, not_end)
    rest(WD, 1)
    for w in (WG, WU, WD):
        comm(w, 2, 0, is_end)
    for k in range(3, F):
        comm(WG, k, 0, is_end)

    @pl.when(is_end)
    def _():
        client_copy(host).wait_send()
        take_back()
        for part in range(2):
            norm_mid(part)
            gather_start(2 + part)

    @pl.when(not_end)
    def _():
        finish_own(0)
        sum_drain(0, 0)
        for part in range(2):
            norm_mid(part)
            gather_start(2 + part)
    for k in range(3, F):
        comm(WU, k, 0, is_end)
        comm(WD, k, 0, is_end)
    arrived(WG)
    arrived(WU)
    for part in range(2):
        hidden_units(t, part)
        ag_c(2 + part, 0, 1 - c).wait_recv()
        hidden_units(x * CORES + 1 - c, part)
    for part in range(2):
        stage = 2 + part
        for o in range(1, X):
            gather_forward_one(stage, o)
            hidden_units(x_peer(X - o) * CORES + c, part)
        for o in range(1, X):
            ag_c(stage, o, 1 - c).wait_recv()
            hidden_units(x_peer(X - o) * CORES + 1 - c, part)
        sums(stage, 0, WD, FH, near + far, wait=part == 0)
    for part in range(2):
        finish_own(2 + part)
        norm_out(part)
        gather_drain(2 + part)
        sum_drain(2 + part, 0)

    @pl.when(is_host)
    def _():
        gather_drain(1)
        sum_drain(1, 1)

        def one(j, _):
            give_back(j, outer).wait_send()
            return 0
        lax.fori_loop(0, F, one, 0)
    for w in range(8):
        drain(w)
    for part in range(PARTS):
        out_copy(part).wait()


def per_device(tokens, norm_gains, *weights):
    G, F, T = lax.axis_size("grp"), lax.axis_size("fs"), lax.axis_size("tp")
    X = T // CORES
    R, D = tokens.shape
    L = R * T
    query, _, value, _, mixer, gate, _, down = weights
    qk_width, v_width, hidden = query.shape[1], value.shape[1], gate.shape[1]
    step = math.gcd(L, 32)
    frequency = np.float32(10000.0) ** (-np.linspace(0.0, 1.0, QK // 2, dtype=np.float32))
    frequency = frequency.astype(np.float64)

    def table(positions):
        angles = positions[:, None] * frequency[None, :]
        return jnp.asarray(np.stack([np.cos(angles), np.sin(angles)]).astype(np.float32))
    vmem = pl.BlockSpec(memory_space=pltpu.VMEM)
    anywhere = pl.BlockSpec(memory_space=pl.ANY)
    DMA = pltpu.SemaphoreType.DMA
    cols = mixer.shape[1]
    scratch = [pltpu.VMEM((w.shape[0] * F, w.shape[1]), bf16) for w in weights]
    scratch += [
        pltpu.VMEM((2, L, D), bf16),
        pltpu.VMEM((2, L, qk_width), bf16),
        pltpu.VMEM((2, L, qk_width), bf16),
        pltpu.VMEM((2, L, max(v_width, hidden)), bf16),
        pltpu.VMEM((2, R, D), f32),
        pltpu.VMEM((2, F, X, R, cols), bf16),
        pltpu.VMEM((2, F, X, R, cols), bf16),
        pltpu.VMEM((2, F, X, R, cols), bf16),
        pltpu.VMEM((L, QK // 2), f32),
        pltpu.VMEM((L, QK // 2), f32),
        pltpu.VMEM((R, D), bf16),
        DMA((8,)),
        DMA((8, F + (F - 1) // 2)), DMA((8, F)),
        DMA((8, F - 1 + (F - 1) // 2, G - 1)), DMA((8, F - 1 + (F - 1) // 2, G - 1)),
        DMA((8, G - 1)), DMA((8, G - 1)),
        DMA((4, X - 1)), DMA((4, X - 1)), DMA((4, X)), DMA((4, X)),
        DMA((4, F)), DMA((4, F)), DMA((4, F, X - 1)), DMA((4, F, X - 1)),
        DMA((2,)), DMA((F,)), DMA((F,)), DMA((4,)),
    ]
    return pl.pallas_call(
        functools.partial(layer, G, F, T),
        out_shape=jax.ShapeDtypeStruct((R, D), bf16),
        in_specs=[vmem] * 4 + [anywhere] * 8,
        out_specs=anywhere,
        scratch_shapes=scratch,
        compiler_params=pltpu.CompilerParams(
            collective_id=0, has_side_effects=True, vmem_limit_bytes=67043328),
    )(tokens, norm_gains, table(np.arange(0.0, L, step)), table(np.arange(0.0, step)), *weights)


def solution(mesh):
    placed = (
        P(("grp", "fs", "tp"), None),
        P(),
        P("fs", "tp"),
        P("fs", "tp"),
        P("fs", "tp"),
        P("fs", "tp"),
        P("tp", "fs"),
        P("fs", "tp"),
        P("fs", "tp"),
        P("tp", "fs"),
    )
    return jax.shard_map(
        per_device,
        mesh=mesh,
        in_specs=placed,
        out_specs=P(("grp", "fs", "tp"), None),
        check_vma=False,
    )
```

```python
import functools
import math

import jax
import jax.numpy as jnp
import numpy as np
from jax import lax
from jax.experimental import pallas as pl
from jax.experimental.pallas import tpu as pltpu
from jax.sharding import PartitionSpec as P

QK = 256
BLOCK = 128
CORES = 2

norm_epsilon = 1e-06
group_epsilon = 0.01

MESH = pl.DeviceIdType.MESH
f32, bf16 = jnp.float32, jnp.bfloat16

WQ, WK, WV, WS, WM, WG, WU, WD = range(8)


def rms(matrix):
    return matrix * lax.rsqrt(jnp.mean(matrix * matrix, axis=-1, keepdims=True) + norm_epsilon)


def silu(value):
    return value / (1.0 + jnp.exp(-value))


def dot(left, right):
    return jnp.dot(left, right, preferred_element_type=f32)


def ds(start, size, multiple=None):
    return pl.ds(pl.multiple_of(start, multiple or size), size)


MIXER = (WQ, WK, WV, WS, WM)
WHOLE = (WQ, WK, WV, WS, WG, WU, WD)


def layer(G, F, T, *refs):
    tokens, gains, coarse, fine = refs[:4]
    shards = refs[4:12]
    out = refs[12]
    bufs = refs[13:21]
    act, queries, keys, values, acc, send1, recv1, recv2 = refs[21:29]
    cosine, sine, rows_out = refs[29:32]
    (local_sem, z_send, z_recv, y_send, y_recv, e_send, e_recv, ag_x_send, ag_x_recv, ag_c_send,
     ag_c_recv, rs1_send, rs1_recv, rs2_send, rs2_recv, client_sem, ret_send, ret_recv, out_sem) = refs[32:]

    X = T // CORES
    g, f, t = lax.axis_index("grp"), lax.axis_index("fs"), lax.axis_index("tp")
    x, c = t // CORES, t % CORES
    R, D = tokens.shape
    L = R * T
    TM = min(256, L)
    heads = queries.shape[2] // QK
    VD = values.shape[2] // heads
    FH = bufs[WG].shape[1]
    total, after = acc.at[0], acc.at[1]
    partner = (g, f, x * CORES + (1 - c))

    moved = F >= 4
    is_end = (f == 0) | (f == F - 1) if moved else f < 0
    is_host = (f == 1) | (f == F - 2) if moved else f < 0
    not_end = jnp.logical_not(is_end)
    outer = jnp.where(f == 1, 0, F - 1)
    host = jnp.where(f == 0, 1, F - 2)

    def x_peer(o):
        return lax.rem(x + o, X)

    neighbours = [(f > 0, (g, f - 1, t)), (f < F - 1, (g, f + 1, t))]
    neighbours += [(None, (lax.rem(g + o, G), f, t)) for o in range(1, G)]
    neighbours += [(None, (g, f, x_peer(o) * CORES + c)) for o in range(1, X)]
    neighbours += [(None, partner)]

    def when(condition, action):
        if condition is None:
            action()
        else:
            pl.when(condition)(action)

    def local_copy(w):
        r = shards[w].shape[0]
        return pltpu.make_async_copy(shards[w], bufs[w].at[ds(f * r, r)], local_sem.at[w])

    def half(w, s, part):
        r = shards[w].shape[0]
        return bufs[w].at[ds(s * r + part * (r // G), r // G)]

    left = f * 2 < F
    ways = (jnp.where(left, 1, 0), jnp.where(left, 0, 1))
    steps = (2 * ways[0] - 1, 2 * ways[1] - 1)

    def source(d, k):
        return f + steps[d] * k

    def target(d):
        return f - steps[d]

    def valid(d, k):
        return (source(d, k) >= 0) & (source(d, k) < F)

    def has_next(w, d):
        margin = 1 if moved and w in MIXER else 0
        return (target(d) >= margin) & (target(d) <= F - 1 - margin)

    def takes(w, k, d):
        return valid(d, k) & not_end if w in MIXER else valid(d, k)

    def gives(w, k, d):
        return has_next(w, d) if k == 0 else takes(w, k, d) & has_next(w, d)

    def from_end(w, k, d):
        return is_host if w in WHOLE and k == 1 and d == 1 else None

    def crosses(w, k, d):
        special = from_end(w, k, d)
        if special is None:
            return takes(w, k, d)
        return takes(w, k, d) & jnp.logical_not(special)

    def z_place(d, k):
        return k if d == 0 else F - 1 + k

    def y_place(d, k):
        return k - 1 if d == 0 else F - 2 + k

    def z_copy(w, k, d):
        region = half(w, source(d, k), g)
        return pltpu.make_async_remote_copy(
            region, region, z_send.at[w, z_place(d, k)], z_recv.at[w, source(d, k)],
            device_id=(g, target(d), t), device_id_type=MESH)

    def z_wait(w, k, d):
        region = half(w, source(d, k), g)
        pltpu.make_async_remote_copy(
            region, region, z_send.at[w, 0], z_recv.at[w, source(d, k)],
            device_id=(g, f, t), device_id_type=MESH).wait_recv()

    def y_copy(w, k, d, o):
        region = half(w, source(d, k), g)
        return pltpu.make_async_remote_copy(
            region, region, y_send.at[w, y_place(d, k), o - 1], y_recv.at[w, y_place(d, k), o - 1],
            device_id=(lax.rem(g + o, G), f, t), device_id_type=MESH)

    def y_wait(w, k, d, o):
        region = half(w, source(d, k), lax.rem(g + G - o, G))
        pltpu.make_async_remote_copy(
            region, region, y_send.at[w, y_place(d, k), o - 1], y_recv.at[w, y_place(d, k), o - 1],
            device_id=(g, f, t), device_id_type=MESH).wait_recv()

    def end_copy(w, o, s, device):
        region = half(w, s, lax.rem(g + o, G))
        return pltpu.make_async_remote_copy(
            region, region, e_send.at[w, o - 1], e_recv.at[w, o - 1],
            device_id=(g, device, t), device_id_type=MESH)

    def give_own(w, early):
        for d in range(2):
            if w in MIXER:
                condition = has_next(w, d)
            elif early:
                condition = is_host if d == 0 else None
            else:
                condition = has_next(w, d)
                if d == 0:
                    condition &= jnp.logical_not(is_host)
            if condition is not None:
                pl.when(condition)(lambda d=d: z_copy(w, 0, d).start())

    def give_rest(w):
        @pl.when(is_end)
        def _():
            for o in range(1, G):
                end_copy(w, o, f, host).start()

    def comm0(w):
        if w in MIXER:
            local_copy(w).wait()
        give_own(w, False)

    def pass_on(w, k, d, who=None):
        if k < F - 1:
            condition = gives(w, k, d)
            pl.when(condition if who is None else condition & who)(
                lambda: z_copy(w, k, d).start())

    def along_z(w, k, d, who=None, onward=True):
        pl.when(takes(w, k, d) if who is None else takes(w, k, d) & who)(
            lambda: z_wait(w, k, d))
        if onward:
            pass_on(w, k, d, who)

    def along_y(w, k, d, who=None):
        @pl.when(crosses(w, k, d) if who is None else crosses(w, k, d) & who)
        def _():
            for o in range(1, G):
                y_copy(w, k, d, o).start()

    def comm(w, k, d, who=None):
        along_z(w, k, d, who)
        along_y(w, k, d, who)

    reach = (range(1, F), range(1, (F - 1) // 2 + 1))

    def rest(w, d, who=None):
        for k in reach[d][1:]:
            comm(w, k, d, who)

    def arrived_from(w, k, d, who=None):
        def narrow(condition):
            return condition if who is None else condition & who

        @pl.when(narrow(crosses(w, k, d)))
        def _():
            for o in range(1, G):
                y_wait(w, k, d, o)
        special = from_end(w, k, d)
        if special is not None:
            @pl.when(narrow(special))
            def _():
                for o in range(1, G):
                    end_copy(w, o, source(d, k), f).wait_recv()

    def arrived(w):
        for d in range(2):
            for k in reach[d]:
                arrived_from(w, k, d)

    def drain(w):
        for d in range(2):
            for k in (0, *reach[d]):
                if k < F - 1:
                    pl.when(gives(w, k, d))(lambda k=k, d=d: z_copy(w, k, d).wait_send())
                if k > 0:
                    @pl.when(crosses(w, k, d))
                    def _(k=k, d=d):
                        for o in range(1, G):
                            y_copy(w, k, d, o).wait_send()
        if w in WHOLE:
            @pl.when(is_end)
            def _():
                for o in range(1, G):
                    end_copy(w, o, f, host).wait_send()

    def rows_of(q, device):
        return act.at[q, ds(device * R, R)]

    def slot(stage):
        return 1 if stage == 1 else 0

    HALF = R // 2

    def window(stage):
        return ds((stage - 2) * HALF, HALF) if stage > 1 else ds(0, R)

    def block_of(stage, device):
        if stage > 1:
            return act.at[0, ds(device * R + (stage - 2) * HALF, HALF)]
        return rows_of(slot(stage), device)

    def ag_x(stage, o):
        region = block_of(stage, t)
        return pltpu.make_async_remote_copy(
            region, region, ag_x_send.at[stage, o - 1], ag_x_recv.at[stage, o - 1],
            device_id=(g, f, x_peer(o) * CORES + c), device_id_type=MESH)

    def ag_c(stage, o, core):
        region = block_of(stage, x_peer(X - o) * CORES + core)
        return pltpu.make_async_remote_copy(
            region, region, ag_c_send.at[stage, o], ag_c_recv.at[stage, o],
            device_id=partner, device_id_type=MESH)

    def gather_start(stage):
        for o in range(1, X):
            ag_x(stage, o).start()
        ag_c(stage, 0, c).start()

    def gather_forward_one(stage, o):
        region = block_of(stage, x_peer(X - o) * CORES + c)
        pltpu.make_async_remote_copy(
            region, region, ag_x_send.at[stage, o - 1], ag_x_recv.at[stage, o - 1],
            device_id=(g, f, t), device_id_type=MESH).wait_recv()
        ag_c(stage, o, c).start()

    def gather_forward(stage):
        for o in range(1, X):
            gather_forward_one(stage, o)

    def gather_wait(stage):
        for o in range(X):
            ag_c(stage, o, 1 - c).wait_recv()

    def gather_drain(stage):
        for o in range(X):
            if o:
                ag_x(stage, o).wait_send()
            ag_c(stage, o, c).wait_send()

    def client_copy(device):
        return pltpu.make_async_remote_copy(
            rows_of(0, t), rows_of(1, t), client_sem.at[0], client_sem.at[1],
            device_id=(g, device, t), device_id_type=MESH)

    cols = send1.shape[-1]

    def rs1(stage, q, j):
        return pltpu.make_async_remote_copy(
            send1.at[q, j, :, window(stage)], recv1.at[q, j, :, window(stage)],
            rs1_send.at[stage, j], rs1_recv.at[stage, j],
            device_id=partner, device_id_type=MESH)

    def rs2(stage, q, j, o):
        return pltpu.make_async_remote_copy(
            send1.at[q, j, o, window(stage)], recv2.at[q, j, o, window(stage)],
            rs2_send.at[stage, j, o - 1], rs2_recv.at[stage, j, o - 1],
            device_id=(g, f, x_peer(o) * CORES + c), device_id_type=MESH)

    def give_back(j, device):
        return pltpu.make_async_remote_copy(
            send1.at[1, j, 0], recv2.at[0, j, 0], ret_send.at[j], ret_recv.at[j],
            device_id=(g, device, t), device_id_type=MESH)

    def partial_rows(stage, w, width, q, j, device):
        r = shards[w].shape[0]
        rows = (ds(device * R + (stage - 2) * HALF, HALF) if stage > 1 else ds(device * R, R))
        return dot(values[q, rows, :width], bufs[w][ds(j * r, r), :])

    def sum_send(stage, q, w, width, j):
        def one(o, _):
            send1[q, j, o, window(stage)] = partial_rows(
                stage, w, width, q, j, o * CORES + (1 - c)).astype(bf16)
            return 0
        lax.fori_loop(0, X, one, 0)
        rs1(stage, q, j).start()

    def sum_pass(stage, q, w, width, j):
        rs1(stage, q, j).wait()
        def pair(o):
            peer = x_peer(o)
            return (partial_rows(stage, w, width, q, j, peer * CORES + c)
                    + recv1[q, j, peer, window(stage)].astype(f32))
        for o in range(1, X):
            send1[q, j, o, window(stage)] = pair(o).astype(bf16)
            rs2(stage, q, j, o).start()
        acc[q, window(stage), ds(j * cols, cols)] = pair(0)

    def sum_finish(stage, q, j):
        block = acc[q, window(stage), ds(j * cols, cols)]
        for o in range(1, X):
            rs2(stage, q, j, o).wait_recv()
            block += recv2[q, j, o, window(stage)].astype(f32)
        return block

    def sum_drain(stage, q):
        def one(j, _):
            for o in range(1, X):
                rs2(stage, q, j, o).wait_send()
            return 0
        lax.fori_loop(0, F, one, 0)

    RT = min(32, R // 2)

    def norm_in():
        def one(i, _):
            rows = ds(i * RT, RT)
            act[0, ds(t * R + i * RT, RT)] = (
                rms(tokens[rows].astype(f32)) * gains[0:1]).astype(bf16)
            return 0
        lax.fori_loop(0, R // RT, one, 0)

    def norm_mid(part):
        def one(i, _):
            rows = ds(i * RT, RT)
            mid = tokens[rows].astype(f32) + rms(total[rows]) * gains[1:2]
            after[rows] = mid
            act[0, ds(t * R + i * RT, RT)] = (rms(mid) * gains[2:3]).astype(bf16)
            return 0
        count = HALF // RT
        lax.fori_loop(part * count, (part + 1) * count, one, 0)

    PARTS = 4

    def out_copy(part):
        rows = ds(part * (R // PARTS), R // PARTS)
        return pltpu.make_async_copy(rows_out.at[rows], out.at[rows], out_sem.at[part])

    def norm_out(half):
        tall = min(RT, R // PARTS)

        def one(i, _):
            rows = ds(i * tall, tall)
            rows_out[rows] = (after[rows] + rms(total[rows]) * gains[3:4]).astype(bf16)
            return 0
        count = R // PARTS // tall
        for part in range(half * PARTS // 2, (half + 1) * PARTS // 2):
            lax.fori_loop(part * count, (part + 1) * count, one, 0)
            out_copy(part).start()

    def tables():
        step = fine.shape[1]

        def one(i, _):
            rows = ds(i * step, step)
            far_cos, far_sin = coarse[0, pl.ds(i, 1)], coarse[1, pl.ds(i, 1)]
            cosine[rows] = far_cos * fine[0] - far_sin * fine[1]
            sine[rows] = far_sin * fine[0] + far_cos * fine[1]
            return 0
        lax.fori_loop(0, L // step, one, 0)

    def tiles(width, tile, body):
        across = width // tile

        tall = min(512, L)

        def one(i, _):
            body(ds((i // across) * tall, tall), ds((i % across) * tile, tile))
            return 0
        lax.fori_loop(0, (L // tall) * across, one, 0)

    def rotary(q, w, into, scale):
        def body(rows, cols):
            head = dot(act[q, rows], bufs[w][:, cols])
            lower, upper = head[:, :QK // 2], head[:, QK // 2:]
            cos, sin = cosine[rows], sine[rows]
            rotated = jnp.concatenate(
                [lower * cos - upper * sin, lower * sin + upper * cos], axis=-1)
            into[q, rows, cols] = (rotated * scale).astype(bf16)
        tiles(heads * QK, QK, body)

    def project_values(q):
        def body(rows, cols):
            values[q, rows, cols] = dot(act[q, rows], bufs[WV][:, cols]).astype(bf16)
        tiles(heads * VD, VD, body)

    def retain(q, h):
        head_index = (t * heads + h).astype(f32)
        fraction = jnp.full((1, 1), 1.0, f32) * (head_index / (heads * T - 1.0))
        log_decay = -(4.0 / BLOCK) * jnp.exp(fraction * math.log(BLOCK / (32.0 * L)))
        qk_cols = ds(h * QK, QK)
        v_cols = ds(h * VD, VD)
        for i in reversed(range(L // TM)):
            rows, seen = pl.ds(i * TM, TM), (i + 1) * TM
            scores = lax.dot_general(
                queries[q, rows, qk_cols], keys[q, :seen, qk_cols], (((1,), (1,)), ((), ())),
                preferred_element_type=f32)
            distance = (lax.broadcasted_iota(jnp.int32, (TM, seen), 0) + i * TM
                        - lax.broadcasted_iota(jnp.int32, (TM, seen), 1)).astype(f32)
            weights = jnp.where(
                distance >= 0, jnp.exp(log_decay * jnp.maximum(distance, 0.0)), 0.0)
            retained = dot((scores * weights).astype(bf16), values[q, :seen, v_cols])
            centred = retained - jnp.mean(retained, axis=-1, keepdims=True)
            normalized = centred * lax.rsqrt(
                jnp.mean(centred * centred, axis=-1, keepdims=True) + group_epsilon)
            values[q, rows, v_cols] = normalized.astype(bf16)

    def retain_all(q):
        lax.fori_loop(0, heads, lambda h, _: (retain(q, h), 0)[1], 0)

    def project_swish(q):
        def body(rows, cols):
            swish = dot(act[q, rows], bufs[WS][:, cols])
            values[q, rows, cols] = (
                silu(swish) * values[q, rows, cols].astype(f32)).astype(bf16)
        tiles(heads * VD, VD, body)

    def hidden_units(device, part):
        tile = math.gcd(FH, 256)

        def one(i, _):
            rows, cols = ds(device * R + part * HALF, HALF), ds(i * tile, tile)
            up = dot(act[0, rows], bufs[WU][:, cols])
            gate = dot(act[0, rows], bufs[WG][:, cols])
            values[0, rows, cols] = (silu(gate) * up).astype(bf16)
            return 0
        lax.fori_loop(0, FH // tile, one, 0)

    def sums(stage, q, w, width, items, who=None, first=None, wait=True):
        def condition(k, d):
            if k == 0:
                return who
            return takes(w, k, d) if who is None else takes(w, k, d) & who

        for n in range(len(items) + 1):
            if n < len(items):
                k, d = items[n]
                if k and wait:
                    arrived_from(w, k, d, first)
                when(condition(k, d), lambda k=k, d=d: sum_send(stage, q, w, width, source(d, k)))
            if n > 0:
                k, d = items[n - 1]
                when(condition(k, d), lambda k=k, d=d: sum_pass(stage, q, w, width, source(d, k)))

    def finish_client(j):
        send1[1, j, 0] = sum_finish(1, 1, j).astype(bf16)
        give_back(j, outer).start()

    def finish_own(stage):
        def one(j, _):
            acc[0, window(stage), ds(j * cols, cols)] = sum_finish(stage, 0, j)
            return 0
        lax.fori_loop(0, F, one, 0)

    def take_back():
        def one(j, _):
            give_back(j, f).wait_recv()
            acc[0, :, ds(j * cols, cols)] = recv2[0, j, 0].astype(f32)
            return 0
        lax.fori_loop(0, F, one, 0)

    far = [(k, d) for k in range(2, F) for d in range(2) if k in reach[d]]
    near = [(0, 0), (1, 0), (1, 1)]
    guest = not_end & jnp.logical_not(is_host)

    for w in range(8):
        local_copy(w).start()
    barrier = pltpu.get_barrier_semaphore()
    for condition, device in neighbours:
        when(condition, lambda device=device: pl.semaphore_signal(
            barrier, inc=1, device_id=device, device_id_type=MESH))
    fixed = (G - 1) + (X - 1) + 1
    pl.semaphore_wait(
        barrier, fixed + (f > 0).astype(jnp.int32) + (f < F - 1).astype(jnp.int32))

    comm0(WQ)
    give_rest(WQ)
    norm_in()
    pl.when(is_end)(lambda: client_copy(host).start())
    pl.when(not_end)(lambda: gather_start(0))
    comm0(WK)
    for w in (WG, WU, WD):
        local_copy(w).wait()
        give_own(w, True)
    pl.when(not_end)(tables)
    comm(WQ, 1, 0)
    comm(WQ, 1, 1)
    rest(WQ, 0)
    rest(WQ, 1)
    comm0(WV)
    comm(WK, 1, 0)

    @pl.when(not_end)
    def _():
        gather_forward(0)
        gather_wait(0)
        arrived(WQ)
        rotary(0, WQ, queries, 1.0)
    comm(WV, 1, 0)
    give_rest(WK)
    comm0(WS)
    give_rest(WV)
    give_rest(WS)

    @pl.when(is_host)
    def _():
        client_copy(f).wait_recv()
        gather_start(1)
    comm(WK, 1, 1)
    rest(WK, 0)
    rest(WK, 1)
    comm(WS, 1, 0)
    comm(WV, 1, 1)
    comm0(WM)

    @pl.when(is_end)
    def _():
        for w in (WG, WU, WD):
            give_own(w, False)
        for w in (WG, WU, WD):
            give_rest(w)

    @pl.when(not_end)
    def _():
        arrived(WK)
        rotary(0, WK, keys, QK ** -0.5)

    @pl.when(is_host)
    def _():
        gather_forward(1)
        gather_wait(1)
        rotary(1, WQ, queries, 1.0)
    rest(WV, 0)
    rest(WV, 1)
    comm(WS, 1, 1)
    pl.when(is_host)(lambda: rotary(1, WK, keys, QK ** -0.5))
    pl.when(not_end)(lambda: arrived(WV))
    pl.when(is_host)(lambda: project_values(1))
    rest(WS, 0)
    rest(WS, 1)

    @pl.when(not_end)
    def _():
        give_own(WG, False)
        give_own(WU, False)
        give_own(WD, False)
    comm(WM, 1, 0)
    pl.when(is_host)(lambda: retain_all(1))
    pl.when(not_end)(lambda: project_values(0))
    along_z(WG, 1, 0)
    along_y(WG, 1, 0, is_end)
    pl.when(not_end)(lambda: retain_all(0))
    pl.when(not_end)(lambda: arrived(WS))
    pl.when(is_host)(lambda: project_swish(1))
    comm(WM, 1, 1)
    along_z(WU, 1, 0)
    along_y(WU, 1, 0, is_end)
    sums(1, 1, WM, heads * VD, near[:2], is_host, is_host)
    comm(WG, 1, 1)
    along_z(WD, 1, 0)
    along_y(WD, 1, 0, is_end)
    pl.when(not_end)(lambda: project_swish(0))
    pl.when(not_end)(lambda: gather_drain(0))
    sums(0, 0, WM, heads * VD, near[:1], not_end, guest)

    @pl.when(is_host)
    def _():
        finish_client(f)
        finish_client(source(0, 1))
    comm(WU, 1, 1)
    rest(WM, 0)
    rest(WM, 1)
    along_y(WG, 1, 0, not_end)
    sums(1, 1, WM, heads * VD, near[2:], is_host, is_host)
    along_y(WU, 1, 0, not_end)
    sums(0, 0, WM, heads * VD, near[1:2], not_end, guest)
    rest(WG, 0, not_end)
    rest(WG, 1)
    comm(WD, 1, 1)
    sums(1, 1, WM, heads * VD, far, is_host, is_host)
    pl.when(is_host)(lambda: finish_client(source(1, 1)))
    sums(0, 0, WM, heads * VD, near[2:] + far, not_end, guest)
    for k in range(2, F):
        along_z(WU, k, 0, not_end, False)
        along_y(WU, k, 0, not_end)
    rest(WU, 1)
    along_y(WD, 1, 0, not_end)
    for k, d in far:
        pl.when(takes(WM, k, d) & is_host)(lambda k=k, d=d: finish_client(source(d, k)))
    for k in range(2, F):
        pass_on(WU, k, 0, not_end)
    rest(WD, 0, not_end)
    rest(WD, 1)
    for w in (WG, WU, WD):
        comm(w, 2, 0, is_end)
    for k in range(3, F):
        comm(WG, k, 0, is_end)

    @pl.when(is_end)
    def _():
        client_copy(host).wait_send()
        take_back()
        for part in range(2):
            norm_mid(part)
            gather_start(2 + part)

    @pl.when(not_end)
    def _():
        finish_own(0)
        sum_drain(0, 0)
        for part in range(2):
            norm_mid(part)
            gather_start(2 + part)
    for k in range(3, F):
        comm(WU, k, 0, is_end)
        comm(WD, k, 0, is_end)
    arrived(WG)
    arrived(WU)
    for part in range(2):
        hidden_units(t, part)
        ag_c(2 + part, 0, 1 - c).wait_recv()
        hidden_units(x * CORES + 1 - c, part)
    for part in range(2):
        stage = 2 + part
        for o in range(1, X):
            gather_forward_one(stage, o)
            hidden_units(x_peer(X - o) * CORES + c, part)
        for o in range(1, X):
            ag_c(stage, o, 1 - c).wait_recv()
            hidden_units(x_peer(X - o) * CORES + 1 - c, part)
        sums(stage, 0, WD, FH, near + far, wait=part == 0)
    for part in range(2):
        finish_own(2 + part)
        norm_out(part)
        gather_drain(2 + part)
        sum_drain(2 + part, 0)

    @pl.when(is_host)
    def _():
        gather_drain(1)
        sum_drain(1, 1)

        def one(j, _):
            give_back(j, outer).wait_send()
            return 0
        lax.fori_loop(0, F, one, 0)
    for w in range(8):
        drain(w)
    for part in range(PARTS):
        out_copy(part).wait()


def per_device(tokens, norm_gains, *weights):
    G, F, T = lax.axis_size("grp"), lax.axis_size("fs"), lax.axis_size("tp")
    X = T // CORES
    R, D = tokens.shape
    L = R * T
    query, _, value, _, mixer, gate, _, down = weights
    qk_width, v_width, hidden = query.shape[1], value.shape[1], gate.shape[1]
    step = math.gcd(L, 32)
    frequency = np.float32(10000.0) ** (-np.linspace(0.0, 1.0, QK // 2, dtype=np.float32))
    frequency = frequency.astype(np.float64)

    def table(positions):
        angles = positions[:, None] * frequency[None, :]
        return jnp.asarray(np.stack([np.cos(angles), np.sin(angles)]).astype(np.float32))
    vmem = pl.BlockSpec(memory_space=pltpu.VMEM)
    anywhere = pl.BlockSpec(memory_space=pl.ANY)
    DMA = pltpu.SemaphoreType.DMA
    cols = mixer.shape[1]
    scratch = [pltpu.VMEM((w.shape[0] * F, w.shape[1]), bf16) for w in weights]
    scratch += [
        pltpu.VMEM((2, L, D), bf16),
        pltpu.VMEM((2, L, qk_width), bf16),
        pltpu.VMEM((2, L, qk_width), bf16),
        pltpu.VMEM((2, L, max(v_width, hidden)), bf16),
        pltpu.VMEM((2, R, D), f32),
        pltpu.VMEM((2, F, X, R, cols), bf16),
        pltpu.VMEM((2, F, X, R, cols), bf16),
        pltpu.VMEM((2, F, X, R, cols), bf16),
        pltpu.VMEM((L, QK // 2), f32),
        pltpu.VMEM((L, QK // 2), f32),
        pltpu.VMEM((R, D), bf16),
        DMA((8,)),
        DMA((8, F + (F - 1) // 2)), DMA((8, F)),
        DMA((8, F - 1 + (F - 1) // 2, G - 1)), DMA((8, F - 1 + (F - 1) // 2, G - 1)),
        DMA((8, G - 1)), DMA((8, G - 1)),
        DMA((4, X - 1)), DMA((4, X - 1)), DMA((4, X)), DMA((4, X)),
        DMA((4, F)), DMA((4, F)), DMA((4, F, X - 1)), DMA((4, F, X - 1)),
        DMA((2,)), DMA((F,)), DMA((F,)), DMA((4,)),
    ]
    return pl.pallas_call(
        functools.partial(layer, G, F, T),
        out_shape=jax.ShapeDtypeStruct((R, D), bf16),
        in_specs=[vmem] * 4 + [anywhere] * 8,
        out_specs=anywhere,
        scratch_shapes=scratch,
        compiler_params=pltpu.CompilerParams(
            collective_id=0, has_side_effects=True, vmem_limit_bytes=67043328),
    )(tokens, norm_gains, table(np.arange(0.0, L, step)), table(np.arange(0.0, step)), *weights)


def solution(mesh):
    placed = (
        P(("grp", "fs", "tp"), None),
        P(),
        P("fs", "tp"),
        P("fs", "tp"),
        P("fs", "tp"),
        P("fs", "tp"),
        P("tp", "fs"),
        P("fs", "tp"),
        P("fs", "tp"),
        P("tp", "fs"),
    )
    return jax.shard_map(
        per_device,
        mesh=mesh,
        in_specs=placed,
        out_specs=P(("grp", "fs", "tp"), None),
        check_vma=False,
    )
```
